512 devices in a mesh: ep: 32 (over z, core), tp: 16 (over y, x).
Axes of the slice: x: 4, y: 4, z: 16, core: 2. Of those that a mesh axis runs over, the one named last changes fastest.
Arguments:
- tokens: bfloat16 [4096, 1024], P('ep', 'tp'), may hold values from -6 to 6
- norm_gain: float32 [1024], replicated, may hold values from 0.1 to 1.9
- gate_weight: bfloat16 [32, 1024, 1024], P('ep', None, 'tp'), may hold values from -0.1875 to 0.1875
- up_weight: bfloat16 [32, 1024, 1024], P('ep', None, 'tp'), may hold values from -0.1875 to 0.1875
- down_weight: bfloat16 [32, 1024, 1024], P('ep', None, 'tp'), may hold values from -0.1875 to 0.1875
- expert_ids: int32 [4096, 4], P('ep'), may hold values from 0 to 31, all different within a row; in each aligned block of 128 rows (0 to 127, 128 to 255, ...) at most 32 rows name the same one
- route_weight: float32 [4096, 4], P('ep'), may hold values from 0.2 to 1
Outputs:
- combined: bfloat16 [4096, 1024], P('ep', 'tp')
The draws below stay inside these ranges and needn't reach their ends.
Inputs may be any that keep to these rules, and one draw needn't show every extreme that they name: `expert_ids`: each token names 4 different experts; in each aligned block of 128 tokens no expert is named by more than 32 of them, and in some block one expert is named by exactly 32; every expert is named by some token.
All inputs are finite; a program needn't handle non-finite values.
Results may differ from the reference program's by a relative error of at most 0.0035.
Values may be sent and summed in bfloat16 or wider, within the bound.
A program may use at most 64 MiB of HBM per device.

```python
import math
import jax
import jax.numpy as jnp
import numpy as np
from jax import lax

D = 1024
FF = 1024
TOPK = 4
TOK_DEV = 128
EXPERTS = 32
TOKENS = 4096
CAP = 32
N_EP = 32


def level_of(key, shape, cuts, low, top_value):
    def one(position, blocks):
        heights = jax.random.uniform(jax.random.fold_in(jax.random.fold_in(key, 6), position), (blocks,), jnp.float32, low / len(cuts), top_value / len(cuts))
        return jnp.repeat(jnp.exp(heights), shape[position] // blocks).reshape((-1,) + (1,) * (len(shape) - position - 1))

    gain = one(*cuts[0])
    for cut in cuts[1:]:
        gain = gain * one(*cut)
    return gain


def deal_out(rng, own, number, rows, amount, top, bound, lean):
    order = jax.random.permutation(rng, amount)
    crowded, usual = shares(amount, rows * top, bound, lean, True), shares(amount, rows * top, bound, lean, False)
    places = jnp.arange(amount)

    def named(sizes, rotation):
        used = int((sizes > 0).sum())
        fixed = max(1, used // 4)
        passed = fixed + (places - fixed + rotation * (used - fixed)) % max(1, amount - fixed)
        return jnp.zeros((amount,), jnp.int32).at[order[jnp.where(places < fixed, places, passed)]].set(jnp.asarray(sizes, jnp.int32))

    sizes = jnp.where(number % 4 == 0, named(crowded, number // 4), named(usual, number - number // 4 - 1))
    mixed = jax.random.permutation(jax.random.fold_in(own, 3), amount)
    giver, taker = mixed[0:amount // 2 * 2:2], mixed[1:amount // 2 * 2:2]
    room = jnp.minimum(sizes[giver] - 1, bound - sizes[taker]) // 2
    room = jnp.where((giver == order[0]) | (taker == order[0]) | (sizes[taker] == 0), 0, jnp.maximum(room, 0))
    passed = jax.random.randint(jax.random.fold_in(own, 4), (amount // 2,), 0, 1 << 20) % (room + 1)
    sizes = sizes.at[giver].add(-passed).at[taker].add(passed)
    members = jnp.searchsorted(jnp.cumsum(sizes), jnp.arange(rows * top), side="right").astype(jnp.int32)
    grid = members.reshape(top, rows).T
    grid = grid[jax.random.permutation(jax.random.fold_in(own, 1), rows)]
    rotation = jax.random.randint(jax.random.fold_in(own, 2), (rows, 1), 0, top)
    return jnp.take_along_axis(grid, (jnp.arange(top)[None, :] + rotation) % top, axis=1)


def shares(number_of, total, most, slope, full):
    weights = [(1 << 20) // math.isqrt(grade ** slope) + 1 for grade in range(1, number_of + 1)]
    largest = most if full else min(most, max(-(-total // number_of), total * weights[0] // sum(weights)))
    least = 1 if total - largest >= number_of - 1 else 0
    given, rest = [largest] + [least] * (number_of - 1), total - largest - least * (number_of - 1)
    while rest > 0:
        free = [i for i in range(1, number_of) if given[i] < largest] or [i for i in range(1, number_of) if given[i] < most]
        pool, left = sum([weights[i] for i in free]), rest
        for i in free:
            extra = min(most - given[i], max(1, left * weights[i] // pool), rest)
            given[i] = given[i] + extra
            rest = rest - extra
    return np.array(given)


def noise(key, shape, scale, most, shards=(), held_as=jnp.bfloat16):
    array = scale * jax.random.normal(key, shape, jnp.float32)
    if shards:
        array = array * level_of(key, shape, shards, -0.22, 0.18)
    return jnp.clip(array, -most, most).astype(held_as)


def setup_inputs(seed: int = 0) -> dict:
    keys = jax.random.split(jax.random.key(seed), 8)
    tokens = noise(keys[0], (TOKENS, D), 1.0, 6.0, ((0, 32), (1, 16)))
    norm_gain = jnp.clip(1.0 + 0.18 * jax.random.normal(keys[1], (D,), jnp.float32), 0.1, 1.9)
    gate_weight = noise(keys[2], (EXPERTS, D, FF), D ** -0.5, 0.1875, ((0, 32), (2, 16)))
    up_weight = noise(keys[3], (EXPERTS, D, FF), D ** -0.5, 0.1875, ((0, 32), (2, 16)))
    down_weight = noise(keys[4], (EXPERTS, FF, D), FF ** -0.5, 0.1875, ((0, 32), (2, 16)))
    expert_ids_keys = jax.random.split(jax.random.fold_in(keys[5], 1), TOKENS // TOK_DEV)
    expert_ids_turns = jax.random.permutation(jax.random.fold_in(keys[5], 3), TOKENS // TOK_DEV)
    expert_ids = jax.vmap(lambda own, number: deal_out(jax.random.fold_in(keys[5], 2), own, number, TOK_DEV, EXPERTS, TOPK, CAP, 2))(expert_ids_keys, expert_ids_turns).reshape((TOKENS, TOPK))
    route_weight = jnp.clip(0.2 + 0.8 * jax.random.uniform(keys[6], (TOKENS, TOPK), jnp.float32) ** level_of(keys[6], (TOKENS, TOPK), ((0, 32),), -0.2, 0.2), 0.2, 1.0)
    return {"tokens": tokens, "norm_gain": norm_gain, "gate_weight": gate_weight, "up_weight": up_weight, "down_weight": down_weight, "expert_ids": expert_ids, "route_weight": route_weight}


epsilon = 1e-06
swish_alpha = 1.702
clamp_limit = 7.0

def rms_normed(values, norm_gain):
    widened = values.astype(jnp.float32)
    scaled = widened * lax.rsqrt(lax.optimization_barrier(jnp.mean(widened * widened, axis=-1, keepdims=True)) + epsilon)
    return (scaled * norm_gain.astype(jnp.float32)).astype(jnp.bfloat16)

def slot_numbers(flat_ids, expert_count):
    selector = (flat_ids[..., None] == jnp.arange(expert_count, dtype=jnp.int32)).astype(jnp.int32)
    before = jnp.cumsum(selector, axis=-2) - selector
    return lax.optimization_barrier(jnp.sum(before * selector, axis=-1)).astype(jnp.int32)

def clamped_units(row_block, w_gate, w_up, w_down):
    gate_pre = jnp.dot(row_block, w_gate, preferred_element_type=jnp.float32)
    up_pre = jnp.dot(row_block, w_up, preferred_element_type=jnp.float32)
    gate_pre = jnp.minimum(gate_pre, clamp_limit)
    up_pre = jnp.clip(up_pre, -clamp_limit, clamp_limit)
    hidden = ((up_pre + 1.0) * gate_pre * jax.nn.sigmoid(swish_alpha * gate_pre)).astype(jnp.bfloat16)
    return jnp.dot(hidden, w_down, preferred_element_type=jnp.float32).astype(jnp.bfloat16)

def reference(tokens, norm_gain, gate_weight, up_weight, down_weight, expert_ids, route_weight):
    normed = rms_normed(tokens, norm_gain)
    assigned = TOK_DEV * TOPK
    flat_ids = expert_ids.reshape(N_EP, assigned).astype(jnp.int32)
    slot_index = slot_numbers(flat_ids, EXPERTS)
    source = jnp.broadcast_to(jnp.arange(N_EP, dtype=jnp.int32)[:, None], (N_EP, assigned))
    owner_token = source * TOK_DEV + jnp.arange(assigned, dtype=jnp.int32)[None, :] // TOPK
    slot_table = jnp.full((EXPERTS, N_EP, CAP), TOKENS, jnp.int32).at[flat_ids, source, slot_index].set(owner_token)
    padded = jnp.concatenate([normed, jnp.zeros((1, D), jnp.bfloat16)], axis=0)

    def one_expert(packed):
        index_table, w_gate, w_up, w_down = packed
        return clamped_units(padded[index_table.reshape(-1)], w_gate, w_up, w_down)
    results = lax.map(one_expert, (slot_table, gate_weight, up_weight, down_weight))
    flat_results = results.reshape(EXPERTS * N_EP * CAP, D)
    locator = ((flat_ids * N_EP + source) * CAP + slot_index).reshape(TOKENS, TOPK)
    picked = flat_results[locator].astype(jnp.float32)
    combined = lax.optimization_barrier(jnp.sum(picked * route_weight.astype(jnp.float32)[:, :, None], axis=1))
    return combined.astype(jnp.bfloat16)
```

```python
import jax
import jax.numpy as jnp
from jax import lax
from jax.experimental import pallas as pl
from jax.experimental.pallas import tpu as pltpu
from jax.sharding import PartitionSpec as P

MESH = pl.DeviceIdType.MESH
F32 = jnp.float32
BF16 = jnp.bfloat16

EPSILON = 1e-06
ALPHA = 1.702
LIMIT = 7.0

NZ = 16
Q = 4
D = 1024
TOK = 128
EXPERTS = 32
TOPK = 4
HALF = 64
Z_ORDER = (8, 7, 9, 6, 10, 5, 11, 4, 12, 3, 13, 2, 14, 1, 15, 0)


def iota(shape, dim):
    return lax.broadcasted_iota(jnp.int32, shape, dim)


def dot(a, b):
    return jnp.dot(a, b, preferred_element_type=F32)


def placed(offset):
    return jnp.where(iota((HALF, 128), 1) == iota((HALF, 128), 0) + offset, 1.0, 0.0).astype(BF16)


def swap(a, b):
    low = iota(a.shape, 1) < HALF
    return jnp.where(low, a, pltpu.roll(b, HALF, 1)), jnp.where(low, pltpu.roll(a, HALF, 1), b)


def kernel(
    tok_hbm, gain_hbm, gate_hbm, up_hbm, down_hbm, ids_hbm, rw_hbm, out_ref,
    tok, gain, gate, up, down, ids, rw,
    pbuf, gub, dnb, dnf, xb, hb, ob, rb,
    in_sem, disp_send, disp_recv, ret_send, ret_recv, ring_send, ring_recv,
):
    ep = lax.axis_index("ep")
    tp = lax.axis_index("tp")
    z, c = ep // 2, ep % 2
    y, x = tp // Q, tp % Q
    x_right, x_left = (x + 1) % Q, (x + 3) % Q
    y_right, y_left = (y + 1) % Q, (y + 3) % Q

    loads = []
    for i, (src, dst) in enumerate(
        ((ids_hbm, ids), (tok_hbm, tok), (gate_hbm.at[0], gate), (up_hbm.at[0], up),
         (down_hbm.at[0], down), (gain_hbm, gain), (rw_hbm, rw))
    ):
        load = pltpu.make_async_copy(src, dst, in_sem.at[i])
        load.start()
        loads.append(load)

    barrier = pltpu.get_barrier_semaphore()

    def greet(device):
        pl.semaphore_signal(barrier, inc=1, device_id=device, device_id_type=MESH)

    for m in range(Q):
        z_from = (z - (m * Q + y) + NZ) % NZ
        for cs in range(2):
            for ys in range(Q):
                device = (z_from * 2 + cs, ys * Q + x)
                if m == 0 and ys == 0:
                    @pl.when(jnp.logical_not(jnp.logical_and(y == 0, c == cs)))
                    def _():
                        greet(device)
                else:
                    greet(device)
    greet((ep, y * Q + x_right))
    greet((ep, y * Q + x_left))
    greet((ep, y_right * Q + x))
    greet((ep, y_left * Q + x))

    loads[0].wait()
    experts = iota((TOK, EXPERTS), 1)
    named = [ids[:, k : k + 1] == experts for k in range(TOPK)]
    member = named[0] | named[1] | named[2] | named[3]
    member_f = jnp.where(member, 1.0, 0.0)
    lower = jnp.where(iota((TOK, TOK), 1) < iota((TOK, TOK), 0), 1.0, 0.0).astype(BF16)
    slot = dot(lower, member_f.astype(BF16))
    code = jnp.where(member, slot, -1.0).astype(BF16)
    expand = jnp.where(iota((EXPERTS, 512), 1) // 16 == iota((EXPERTS, 512), 0), 1.0, 0.0).astype(BF16)
    code_wide = dot(code, expand)
    place = (iota((TOK, 512), 1) % 16).astype(F32)
    pick_low = jnp.where(code_wide == place, 1.0, 0.0)
    pick_high = jnp.where(code_wide == place + 16.0, 1.0, 0.0)

    left_eye, right_eye = placed(0), placed(HALF)
    loads[1].wait()
    token_low = dot(tok[...], left_eye).astype(BF16)
    token_high = dot(tok[...], right_eye).astype(BF16)
    first = (((0,), (0,)), ((), ()))
    packed = lax.dot_general(
        pick_low.astype(BF16), token_low, first, preferred_element_type=F32
    ) + lax.dot_general(pick_high.astype(BF16), token_high, first, preferred_element_type=F32)
    pbuf[...] = packed.astype(BF16)

    loads[2].wait()
    loads[3].wait()
    gub[y] = (dot(gate[...], left_eye) + dot(up[...], right_eye)).astype(BF16)
    loads[4].wait()
    dnb[y] = (dot(down[0:512, :], left_eye) + dot(down[512:1024, :], right_eye)).astype(BF16)

    own_edge = jnp.where(y == 0, 1, 0)
    pl.semaphore_wait(barrier, 2 * NZ + 4 - own_edge)

    sends = []
    for dz in Z_ORDER:
        m, yd = dz // Q, dz % Q
        for ce in range(2):
            e = ((z + dz) % NZ) * 2 + ce
            copy = pltpu.make_async_remote_copy(
                src_ref=pbuf.at[pl.ds(pl.multiple_of(e * 16, 16), 16)],
                dst_ref=xb.at[x, y, pl.ds(pl.multiple_of((m * 2 + c) * 16, 16), 16)],
                send_sem=disp_send.at[dz * 2 + ce],
                recv_sem=disp_recv.at[(m * 2 + c) * Q + y],
                device_id=(e, yd * Q + x),
                device_id_type=MESH,
            )
            if dz == 0:
                own = jnp.logical_and(y == 0, c == ce)

                @pl.when(jnp.logical_not(own))
                def _():
                    copy.start()

                @pl.when(own)
                def _():
                    xb[x, 0, pl.ds(pl.multiple_of(c * 16, 16), 16), :] = pbuf[
                        pl.ds(pl.multiple_of(e * 16, 16), 16), :
                    ]
                sends.append((copy, own))
            else:
                copy.start()
                sends.append((copy, None))

    class Ring:
        def __init__(self, buf, half, mine, right, left, device, base):
            self.buf, self.half, self.mine, self.base = buf, half, mine, base
            self.right, self.left, self.device = right, left, device
            self.sent = []

        def part(self, owner, h):
            return self.buf.at[owner, pl.ds(h * self.half, self.half)]

        def copy(self, owner, h, to, index):
            return pltpu.make_async_remote_copy(
                src_ref=self.part(owner, h),
                dst_ref=self.part(owner, h),
                send_sem=ring_send.at[self.base + index],
                recv_sem=ring_recv.at[self.base + index],
                device_id=self.device(to),
                device_id_type=MESH,
            )

        def send(self, owner, h, to, index):
            copy = self.copy(owner, h, to, index)
            copy.start()
            self.sent.append(copy)

        def arrived(self, owner, h, index):
            self.copy(owner, h, self.right, index).wait_recv()

        def start(self):
            self.send(self.mine, 0, self.right, 0)
            self.send(self.mine, 1, self.left, 1)
            self.send(self.mine, 1, self.right, 2)
            self.send(self.mine, 0, self.left, 3)

        def forward(self):
            self.arrived(self.left, 0, 0)
            self.send(self.left, 0, self.right, 4)
            self.arrived(self.right, 1, 1)
            self.send(self.right, 1, self.left, 5)

        def finish(self):
            far = (self.mine + 2) % Q
            self.arrived(self.left, 1, 2)
            self.arrived(self.right, 0, 3)
            self.arrived(far, 0, 4)
            self.arrived(far, 1, 5)

        def drain(self):
            for copy in self.sent:
                copy.wait_send()

    def along_x(to):
        return (ep, y * Q + to)

    def along_y(to):
        return (ep, to * Q + x)

    gu_ring = Ring(gub, 512, y, y_right, y_left, along_y, 0)
    dn_ring = Ring(dnb, 256, y, y_right, y_left, along_y, 6)
    x_ring = Ring(xb, 2, x, x_right, x_left, along_x, 12)
    h_ring = Ring(hb, 1, x, x_right, x_left, along_x, 18)

    gu_ring.start()
    gu_ring.forward()
    dn_ring.start()

    def dispatch_arrived(m, cs, ys):
        pltpu.make_async_remote_copy(
            src_ref=pbuf.at[pl.ds(0, 16)],
            dst_ref=xb.at[x, ys, pl.ds((m * 2 + cs) * 16, 16)],
            send_sem=disp_send.at[0],
            recv_sem=disp_recv.at[(m * 2 + cs) * Q + ys],
            device_id=(ep, tp),
            device_id_type=MESH,
        ).wait_recv()

    for m in range(Q):
        for cs in range(2):
            for ys in range(Q):
                if m == 0 and ys == 0:
                    @pl.when(jnp.logical_not(jnp.logical_and(y == 0, c == cs)))
                    def _():
                        dispatch_arrived(m, cs, ys)
                else:
                    dispatch_arrived(m, cs, ys)

    x_ring.start()
    x_ring.forward()
    dn_ring.forward()
    x_ring.finish()

    loads[5].wait()
    loads[6].wait()
    groups = []
    square = jnp.zeros((256, 128), F32)
    for g in range(8):
        ys, xs = g // 2, (g % 2) * 2
        low, high = swap(xb[xs, ys].astype(F32), xb[xs + 1, ys].astype(F32))
        part = jnp.concatenate([low, high], axis=0)
        square = square + part * part
        groups.append(part)
    inverse = lax.rsqrt(jnp.sum(square, axis=1, keepdims=True) / D + EPSILON)
    rows = jnp.concatenate(
        [(groups[g] * inverse * gain[g : g + 1, :]).astype(BF16) for g in range(8)], axis=1
    )

    gu_ring.finish()
    for p in range(2):
        both = dot(rows, jnp.concatenate([gub[2 * p], gub[2 * p + 1]], axis=1))
        gate_pre, up_pre = swap(both[:, :128], both[:, 128:])
        gate_pre = jnp.minimum(gate_pre, LIMIT)
        up_pre = jnp.clip(up_pre, -LIMIT, LIMIT)
        hidden = (up_pre + 1.0) * gate_pre * jax.nn.sigmoid(ALPHA * gate_pre)
        hb[x, p] = hidden.astype(BF16)
    h_ring.start()
    h_ring.forward()

    dn_ring.finish()
    for n in range(2):
        low, high = swap(dnb[2 * n].astype(F32), dnb[2 * n + 1].astype(F32))
        for xs in range(Q):
            for p in range(2):
                for h in range(2):
                    src = (low, high)[p][HALF * (4 * h + xs) : HALF * (4 * h + xs) + HALF]
                    at = (xs * 2 + p) * 128 + h * HALF
                    dnf[at : at + HALF, n * 128 : n * 128 + 128] = src.astype(BF16)

    h_ring.finish()
    hidden_all = jnp.concatenate([hb[k // 2, k % 2] for k in range(8)], axis=1)
    result = dot(hidden_all, dnf[...])
    for n in range(2):
        cols = result[:, n * 128 : n * 128 + 128]
        ob[2 * n], ob[2 * n + 1] = [v.astype(BF16) for v in swap(cols[:128], cols[128:])]

    for m in (2, 1, 3, 0):
        z_to = (z - (m * Q + y) + NZ) % NZ
        for cs in range(2):
            for ys in range(Q):
                copy = pltpu.make_async_remote_copy(
                    src_ref=ob.at[ys, pl.ds((m * 2 + cs) * 16, 16)],
                    dst_ref=rb.at[pl.ds(pl.multiple_of(ep * 16, 16), 16)],
                    send_sem=ret_send.at[(m * 2 + cs) * Q + ys],
                    recv_sem=ret_recv.at[ep],
                    device_id=(z_to * 2 + cs, ys * Q + x),
                    device_id_type=MESH,
                )
                if m == 0 and ys == 0:
                    own = jnp.logical_and(y == 0, c == cs)

                    @pl.when(jnp.logical_not(own))
                    def _():
                        copy.start()

                    @pl.when(own)
                    def _():
                        rb[pl.ds(pl.multiple_of(ep * 16, 16), 16), :] = ob[
                            0, cs * 16 : cs * 16 + 16, :
                        ]
                    sends.append((copy, own))
                else:
                    copy.start()
                    sends.append((copy, None))

    weight = jnp.zeros((TOK, EXPERTS), F32)
    for k in range(TOPK):
        weight = weight + jnp.where(named[k], rw[:, k : k + 1], 0.0)
    stack = []
    for pick in (pick_low, pick_high):
        rest = weight
        for _ in range(3):
            piece = rest.astype(BF16)
            rest = rest - piece.astype(F32)
            stack.append((dot(piece, expand) * pick).astype(BF16))
    mixer = jnp.concatenate(stack, axis=0)

    for dz in range(NZ):
        for ce in range(2):
            e = ((z + dz) % NZ) * 2 + ce
            arrived = pltpu.make_async_remote_copy(
                src_ref=ob.at[0, pl.ds(0, 16)],
                dst_ref=rb.at[pl.ds(pl.multiple_of(e * 16, 16), 16)],
                send_sem=ret_send.at[0],
                recv_sem=ret_recv.at[e],
                device_id=(ep, tp),
                device_id_type=MESH,
            )
            if dz == 0:
                @pl.when(jnp.logical_not(jnp.logical_and(y == 0, c == ce)))
                def _():
                    arrived.wait_recv()
            else:
                arrived.wait_recv()

    mixed = dot(mixer, rb[...])
    from_low = mixed[0:128] + mixed[128:256] + mixed[256:384]
    from_high = mixed[384:512] + mixed[512:640] + mixed[640:768]
    combined = from_low + pltpu.roll(from_high, HALF, 1)
    out_ref[...] = combined[:, :HALF].astype(BF16)

    for copy, own in sends:
        if own is None:
            copy.wait_send()
        else:
            @pl.when(jnp.logical_not(own))
            def _():
                copy.wait_send()
    for ring in (gu_ring, dn_ring, x_ring, h_ring):
        ring.drain()


def body(tokens, norm_gain, gate_weight, up_weight, down_weight, expert_ids, route_weight):
    return pl.pallas_call(
        kernel,
        out_shape=jax.ShapeDtypeStruct((TOK, HALF), BF16),
        in_specs=[pl.BlockSpec(memory_space=pl.ANY)] * 7,
        out_specs=pl.BlockSpec(memory_space=pltpu.VMEM),
        scratch_shapes=[
            pltpu.VMEM((TOK, HALF), BF16),
            pltpu.VMEM((8, 128), F32),
            pltpu.VMEM((D, HALF), BF16),
            pltpu.VMEM((D, HALF), BF16),
            pltpu.VMEM((D, HALF), BF16),
            pltpu.VMEM((TOK, TOPK), jnp.int32),
            pltpu.VMEM((TOK, TOPK), F32),
            pltpu.VMEM((512, 128), BF16),
            pltpu.VMEM((Q, D, 128), BF16),
            pltpu.VMEM((Q, 512, 128), BF16),
            pltpu.VMEM((D, 256), BF16),
            pltpu.VMEM((Q, Q, 128, 128), BF16),
            pltpu.VMEM((Q, 2, 256, 128), BF16),
            pltpu.VMEM((Q, 128, 128), BF16),
            pltpu.VMEM((512, 128), BF16),
            pltpu.SemaphoreType.DMA((7,)),
            pltpu.SemaphoreType.DMA((32,)),
            pltpu.SemaphoreType.DMA((32,)),
            pltpu.SemaphoreType.DMA((32,)),
            pltpu.SemaphoreType.DMA((32,)),
            pltpu.SemaphoreType.DMA((24,)),
            pltpu.SemaphoreType.DMA((24,)),
        ],
        compiler_params=pltpu.CompilerParams(collective_id=0, has_side_effects=True),
    )(
        tokens, norm_gain.reshape(8, 128), gate_weight, up_weight, down_weight,
        expert_ids, route_weight,
    )


def solution(mesh):
    in_specs = (
        P("ep", "tp"),
        P(),
        P("ep", None, "tp"),
        P("ep", None, "tp"),
        P("ep", None, "tp"),
        P("ep", None),
        P("ep", None),
    )
    return jax.shard_map(body, mesh=mesh, in_specs=in_specs, out_specs=P("ep", "tp"), check_vma=False)
```

```python
import jax
import jax.numpy as jnp
from jax import lax
from jax.experimental import pallas as pl
from jax.experimental.pallas import tpu as pltpu
from jax.sharding import PartitionSpec as P

MESH = pl.DeviceIdType.MESH
F32 = jnp.float32
BF16 = jnp.bfloat16

EPSILON = 1e-06
ALPHA = 1.702
LIMIT = 7.0

NZ = 16
Q = 4
D = 1024
TOK = 128
EXPERTS = 32
TOPK = 4
HALF = 64
Z_ORDER = (8, 7, 9, 6, 10, 5, 11, 4, 12, 3, 13, 2, 14, 1, 15, 0)


def iota(shape, dim):
    return lax.broadcasted_iota(jnp.int32, shape, dim)


def dot(a, b):
    return jnp.dot(a, b, preferred_element_type=F32)


def dot_rows(a, b):
    return lax.dot_general(a, b, (((1,), (1,)), ((), ())), preferred_element_type=F32)


def dot_columns(a, b):
    return lax.dot_general(a, b, (((0,), (0,)), ((), ())), preferred_element_type=F32)


def placed(offset):
    return jnp.where(iota((HALF, 128), 1) == iota((HALF, 128), 0) + offset, 1.0, 0.0).astype(BF16)


def swap(a, b):
    low = iota(a.shape, 1) < HALF
    return jnp.where(low, a, pltpu.roll(b, HALF, 1)), jnp.where(low, pltpu.roll(a, HALF, 1), b)


def kernel(
    tok_hbm, gain_hbm, gate_hbm, up_hbm, down_hbm, ids_hbm, rw_hbm, out_ref,
    tok, gain, ids, rw,
    pbuf, gub, dnb, dnf, xb, hb, ob, rb, mixer,
    in_sem, disp_send, disp_recv, ret_send, ret_recv, ring_send, ring_recv,
):
    ep = lax.axis_index("ep")
    tp = lax.axis_index("tp")
    z, c = ep // 2, ep % 2
    y, x = tp // Q, tp % Q
    x_right, x_left = (x + 1) % Q, (x + 3) % Q
    y_right, y_left = (y + 1) % Q, (y + 3) % Q

    loads = []
    for i, (src, dst) in enumerate(
        ((ids_hbm, ids), (tok_hbm, tok), (gate_hbm.at[0], gub.at[y, pl.ds(0, HALF)]),
         (up_hbm.at[0], gub.at[y, pl.ds(HALF, HALF)]), (down_hbm.at[0], dnb.at[y]),
         (gain_hbm, gain), (rw_hbm, rw))
    ):
        load = pltpu.make_async_copy(src, dst, in_sem.at[i])
        load.start()
        loads.append(load)

    barrier = pltpu.get_barrier_semaphore()

    def greet(device):
        pl.semaphore_signal(barrier, inc=1, device_id=device, device_id_type=MESH)

    for m in range(Q):
        z_from = (z - (m * Q + y) + NZ) % NZ
        for cs in range(2):
            for ys in range(Q):
                device = (z_from * 2 + cs, ys * Q + x)
                if m == 0 and ys == 0:
                    @pl.when(jnp.logical_not(jnp.logical_and(y == 0, c == cs)))
                    def _():
                        greet(device)
                else:
                    greet(device)
    greet((ep, y * Q + x_right))
    greet((ep, y * Q + x_left))
    greet((ep, y_right * Q + x))
    greet((ep, y_left * Q + x))

    loads[0].wait()
    experts = iota((EXPERTS, TOK), 0)
    named = [ids[k : k + 1, :] == experts for k in range(TOPK)]
    member = named[0] | named[1] | named[2] | named[3]
    earlier = jnp.where(iota((TOK, TOK), 0) < iota((TOK, TOK), 1), 1.0, 0.0).astype(BF16)
    slot = dot(jnp.where(member, 1.0, 0.0).astype(BF16), earlier)
    code = jnp.where(member, slot, -1.0).astype(BF16)
    expand = jnp.where(iota((512, EXPERTS), 0) // 16 == iota((512, EXPERTS), 1), 1.0, 0.0).astype(BF16)
    code_wide = dot(expand, code)
    place = (iota((512, TOK), 0) % 16).astype(F32)
    pick_low = jnp.where(code_wide == place, 1.0, 0.0)
    pick_high = jnp.where(code_wide == place + 16.0, 1.0, 0.0)

    loads[1].wait()
    token_low = dot_columns(tok[...], placed(0)).astype(BF16)
    token_high = dot_columns(tok[...], placed(HALF)).astype(BF16)
    packed = dot(pick_low.astype(BF16), token_low) + dot(pick_high.astype(BF16), token_high)
    pbuf[...] = packed.astype(BF16)

    loads[6].wait()
    weight = jnp.zeros((EXPERTS, TOK), F32)
    for k in range(TOPK):
        weight = weight + jnp.where(named[k], rw[k : k + 1, :], 0.0)
    for i in range(3):
        piece = weight.astype(BF16)
        weight = weight - piece.astype(F32)
        wide = dot(expand, piece)
        mixer[:, i * 128 : i * 128 + 128] = (wide * pick_low).astype(BF16)
        mixer[:, 384 + i * 128 : 512 + i * 128] = (wide * pick_high).astype(BF16)

    for load in loads[2:6]:
        load.wait()
    own_edge = jnp.where(y == 0, 1, 0)
    pl.semaphore_wait(barrier, 2 * NZ + 4 - own_edge)

    sends = []
    for dz in Z_ORDER:
        m, yd = dz // Q, dz % Q
        for ce in range(2):
            e = ((z + dz) % NZ) * 2 + ce
            copy = pltpu.make_async_remote_copy(
                src_ref=pbuf.at[pl.ds(pl.multiple_of(e * 16, 16), 16)],
                dst_ref=xb.at[x, y, pl.ds(pl.multiple_of((m * 2 + c) * 16, 16), 16)],
                send_sem=disp_send.at[dz * 2 + ce],
                recv_sem=disp_recv.at[(m * 2 + c) * Q + y],
                device_id=(e, yd * Q + x),
                device_id_type=MESH,
            )
            if dz == 0:
                own = jnp.logical_and(y == 0, c == ce)

                @pl.when(jnp.logical_not(own))
                def _():
                    copy.start()

                @pl.when(own)
                def _():
                    xb[x, 0, pl.ds(pl.multiple_of(c * 16, 16), 16), :] = pbuf[
                        pl.ds(pl.multiple_of(e * 16, 16), 16), :
                    ]
                sends.append((copy, own))
            else:
                copy.start()
                sends.append((copy, None))

    class Ring:
        def __init__(self, buf, half, mine, right, left, device, base):
            self.buf, self.half, self.mine, self.base = buf, half, mine, base
            self.right, self.left, self.device = right, left, device
            self.sent = []

        def part(self, owner, h):
            return self.buf.at[owner, pl.ds(h * self.half, self.half)]

        def copy(self, owner, h, to, index):
            return pltpu.make_async_remote_copy(
                src_ref=self.part(owner, h),
                dst_ref=self.part(owner, h),
                send_sem=ring_send.at[self.base + index],
                recv_sem=ring_recv.at[self.base + index],
                device_id=self.device(to),
                device_id_type=MESH,
            )

        def send(self, owner, h, to, index):
            copy = self.copy(owner, h, to, index)
            copy.start()
            self.sent.append(copy)

        def arrived(self, owner, h, index):
            self.copy(owner, h, self.right, index).wait_recv()

        def start(self):
            self.send(self.mine, 0, self.right, 0)
            self.send(self.mine, 1, self.left, 1)
            self.send(self.mine, 1, self.right, 2)
            self.send(self.mine, 0, self.left, 3)

        def forward(self):
            self.arrived(self.left, 0, 0)
            self.send(self.left, 0, self.right, 4)
            self.arrived(self.right, 1, 1)
            self.send(self.right, 1, self.left, 5)

        def finish(self):
            far = (self.mine + 2) % Q
            self.arrived(self.left, 1, 2)
            self.arrived(self.right, 0, 3)
            self.arrived(far, 0, 4)
            self.arrived(far, 1, 5)

        def drain(self):
            for copy in self.sent:
                copy.wait_send()

    def along_x(to):
        return (ep, y * Q + to)

    def along_y(to):
        return (ep, to * Q + x)

    gu_ring = Ring(gub, 64, y, y_right, y_left, along_y, 0)
    dn_ring = Ring(dnb, 32, y, y_right, y_left, along_y, 6)
    x_ring = Ring(xb, 2, x, x_right, x_left, along_x, 12)
    h_ring = Ring(hb, 1, x, x_right, x_left, along_x, 18)

    gu_ring.start()
    gu_ring.forward()
    dn_ring.start()

    def dispatch_arrived(m, cs, ys):
        pltpu.make_async_remote_copy(
            src_ref=pbuf.at[pl.ds(0, 16)],
            dst_ref=xb.at[x, ys, pl.ds((m * 2 + cs) * 16, 16)],
            send_sem=disp_send.at[0],
            recv_sem=disp_recv.at[(m * 2 + cs) * Q + ys],
            device_id=(ep, tp),
            device_id_type=MESH,
        ).wait_recv()

    for m in range(Q):
        for cs in range(2):
            for ys in range(Q):
                if m == 0 and ys == 0:
                    @pl.when(jnp.logical_not(jnp.logical_and(y == 0, c == cs)))
                    def _():
                        dispatch_arrived(m, cs, ys)
                else:
                    dispatch_arrived(m, cs, ys)

    x_ring.start()
    x_ring.forward()
    dn_ring.forward()
    x_ring.finish()

    groups = []
    square = jnp.zeros((256, 128), F32)
    for g in range(8):
        ys, xs = g // 2, (g % 2) * 2
        low, high = swap(xb[xs, ys].astype(F32), xb[xs + 1, ys].astype(F32))
        part = jnp.concatenate([low, high], axis=0)
        square = square + part * part
        groups.append(part)
    inverse = lax.rsqrt(jnp.sum(square, axis=1, keepdims=True) / D + EPSILON)
    rows = jnp.concatenate(
        [(groups[g] * inverse * gain[g : g + 1, :]).astype(BF16) for g in range(8)], axis=1
    )

    gu_ring.finish()
    for p in range(2):
        both = dot_rows(rows, jnp.concatenate([gub[2 * p], gub[2 * p + 1]], axis=0))
        gate_pre, up_pre = swap(both[:, :128], both[:, 128:])
        gate_pre = jnp.minimum(gate_pre, LIMIT)
        up_pre = jnp.clip(up_pre, -LIMIT, LIMIT)
        hidden = (up_pre + 1.0) * gate_pre * jax.nn.sigmoid(ALPHA * gate_pre)
        hb[x, p] = hidden.astype(BF16)
    h_ring.start()
    h_ring.forward()

    dn_ring.finish()
    for n in range(Q):
        for p in range(2):
            for m in range(2):
                g = (4 * p + m) * 128
                even, odd = swap(
                    dnb[n, :, g : g + 128].astype(F32), dnb[n, :, g + 256 : g + 384].astype(F32)
                )
                at = (4 * m + p) * 128
                dnf[n * HALF : n * HALF + HALF, at : at + 128] = even.astype(BF16)
                dnf[n * HALF : n * HALF + HALF, at + 256 : at + 384] = odd.astype(BF16)

    h_ring.finish()
    hidden_all = jnp.concatenate([hb[k // 2, k % 2] for k in range(8)], axis=1)
    result = dot_rows(hidden_all, dnf[...])
    for n in range(2):
        cols = result[:, n * 128 : n * 128 + 128]
        ob[2 * n], ob[2 * n + 1] = [v.astype(BF16) for v in swap(cols[:128], cols[128:])]

    for m in (2, 1, 3, 0):
        z_to = (z - (m * Q + y) + NZ) % NZ
        for cs in range(2):
            for ys in range(Q):
                copy = pltpu.make_async_remote_copy(
                    src_ref=ob.at[ys, pl.ds((m * 2 + cs) * 16, 16)],
                    dst_ref=rb.at[pl.ds(pl.multiple_of(ep * 16, 16), 16)],
                    send_sem=ret_send.at[(m * 2 + cs) * Q + ys],
                    recv_sem=ret_recv.at[ep],
                    device_id=(z_to * 2 + cs, ys * Q + x),
                    device_id_type=MESH,
                )
                if m == 0 and ys == 0:
                    own = jnp.logical_and(y == 0, c == cs)

                    @pl.when(jnp.logical_not(own))
                    def _():
                        copy.start()

                    @pl.when(own)
                    def _():
                        rb[pl.ds(pl.multiple_of(ep * 16, 16), 16), :] = ob[
                            0, cs * 16 : cs * 16 + 16, :
                        ]
                    sends.append((copy, own))
                else:
                    copy.start()
                    sends.append((copy, None))

    for dz in range(NZ):
        for ce in range(2):
            e = ((z + dz) % NZ) * 2 + ce
            arrived = pltpu.make_async_remote_copy(
                src_ref=ob.at[0, pl.ds(0, 16)],
                dst_ref=rb.at[pl.ds(pl.multiple_of(e * 16, 16), 16)],
                send_sem=ret_send.at[0],
                recv_sem=ret_recv.at[e],
                device_id=(ep, tp),
                device_id_type=MESH,
            )
            if dz == 0:
                @pl.when(jnp.logical_not(jnp.logical_and(y == 0, c == ce)))
                def _():
                    arrived.wait_recv()
            else:
                arrived.wait_recv()

    mixed = dot_columns(rb[...], mixer[...])
    combined = mixed[0:HALF, 0:128] + mixed[HALF:128, 384:512]
    for i in range(1, 3):
        combined = combined + mixed[0:HALF, i * 128 : i * 128 + 128]
        combined = combined + mixed[HALF:128, 384 + i * 128 : 512 + i * 128]
    out_ref[...] = combined.astype(BF16)

    for copy, own in sends:
        if own is None:
            copy.wait_send()
        else:
            @pl.when(jnp.logical_not(own))
            def _():
                copy.wait_send()
    for ring in (gu_ring, dn_ring, x_ring, h_ring):
        ring.drain()


def body(tokens, norm_gain, gate_weight, up_weight, down_weight, expert_ids, route_weight):
    turned = (0, 2, 1)
    return pl.pallas_call(
        kernel,
        out_shape=jax.ShapeDtypeStruct((HALF, TOK), BF16),
        in_specs=[pl.BlockSpec(memory_space=pl.ANY)] * 7,
        out_specs=pl.BlockSpec(memory_space=pltpu.VMEM),
        scratch_shapes=[
            pltpu.VMEM((HALF, TOK), BF16),
            pltpu.VMEM((8, 128), F32),
            pltpu.VMEM((TOPK, TOK), jnp.int32),
            pltpu.VMEM((TOPK, TOK), F32),
            pltpu.VMEM((512, 128), BF16),
            pltpu.VMEM((Q, 128, D), BF16),
            pltpu.VMEM((Q, HALF, D), BF16),
            pltpu.VMEM((256, D), BF16),
            pltpu.VMEM((Q, Q, 128, 128), BF16),
            pltpu.VMEM((Q, 2, 256, 128), BF16),
            pltpu.VMEM((Q, 128, 128), BF16),
            pltpu.VMEM((512, 128), BF16),
            pltpu.VMEM((512, 768), BF16),
            pltpu.SemaphoreType.DMA((7,)),
            pltpu.SemaphoreType.DMA((32,)),
            pltpu.SemaphoreType.DMA((32,)),
            pltpu.SemaphoreType.DMA((32,)),
            pltpu.SemaphoreType.DMA((32,)),
            pltpu.SemaphoreType.DMA((24,)),
            pltpu.SemaphoreType.DMA((24,)),
        ],
        compiler_params=pltpu.CompilerParams(collective_id=0, has_side_effects=True),
    )(
        tokens.T, norm_gain.reshape(8, 128), gate_weight.transpose(turned), up_weight.transpose(turned),
        down_weight.transpose(turned), expert_ids.T, route_weight.T,
    ).T


def solution(mesh):
    in_specs = (
        P("ep", "tp"),
        P(),
        P("ep", None, "tp"),
        P("ep", None, "tp"),
        P("ep", None, "tp"),
        P("ep", None),
        P("ep", None),
    )
    return jax.shard_map(body, mesh=mesh, in_specs=in_specs, out_specs=P("ep", "tp"), check_vma=False)
```

```python
import jax
import jax.numpy as jnp
from jax import lax
from jax.experimental import pallas as pl
from jax.experimental.pallas import tpu as pltpu
from jax.sharding import PartitionSpec as P

MESH = pl.DeviceIdType.MESH
F32 = jnp.float32
BF16 = jnp.bfloat16

EPSILON = 1e-06
ALPHA = 1.702
LIMIT = 7.0

NZ = 16
Q = 4
D = 1024
TOK = 128
EXPERTS = 32
TOPK = 4
HALF = 64
Z_ORDER = (8, 7, 9, 6, 10, 5, 11, 4, 12, 3, 13, 2, 14, 1, 15, 0)
PARTS = ((0, 3), (1, 2))
M_AT = {m: i for i, m in enumerate(m for part in PARTS for m in part)}
N_PART = len(PARTS)
PACKED = 128 // N_PART


def iota(shape, dim):
    return lax.broadcasted_iota(jnp.int32, shape, dim)


def dot(a, b):
    return jnp.dot(a, b, preferred_element_type=F32)


def dot_rows(a, b):
    return lax.dot_general(a, b, (((1,), (1,)), ((), ())), preferred_element_type=F32)


def dot_columns(a, b):
    return lax.dot_general(a, b, (((0,), (0,)), ((), ())), preferred_element_type=F32)


def placed(offset):
    return jnp.where(iota((HALF, 128), 1) == iota((HALF, 128), 0) + offset, 1.0, 0.0).astype(BF16)


def swap(a, b):
    low = iota(a.shape, 1) < HALF
    return jnp.where(low, a, pltpu.roll(b, HALF, 1)), jnp.where(low, pltpu.roll(a, HALF, 1), b)


def bits(v):
    return v // 2, ((v + 1) % Q) // 2


def gray(a, b):
    return 3 * a + b - 2 * a * b


def place(k, quarter, column):
    if isinstance(k, int):
        a, b = (quarter, column) if k == 0 else (column, quarter)
    else:
        a = quarter + k * (column - quarter)
        b = column + k * (quarter - column)
    return gray(a // 2, b // 2) * Q + gray(a % 2, b % 2)


def rows_at(m, core):
    return (M_AT[m] * 2 + core) * 16


def tile(start):
    return pl.ds(start if isinstance(start, int) else pl.multiple_of(start, 16), 16)


class Gather:
    def __init__(self, view, mine, device, sems, base):
        self.view, self.device, self.base = view, device, base
        self.send_sems, self.recv_sems = sems
        self.mine = mine
        self.right = mine + 1 - 2 * (mine % 2)
        self.left = mine + 2 - 4 * (mine // 2)
        self.far = 3 - mine
        self.sent = []

    def copy(self, owner, h, to, index):
        return pltpu.make_async_remote_copy(
            src_ref=self.view(owner, h),
            dst_ref=self.view(owner, h),
            send_sem=self.send_sems.at[self.base + index],
            recv_sem=self.recv_sems.at[self.base + index],
            device_id=self.device(to),
            device_id_type=MESH,
        )

    def send(self, owner, h, to, index):
        copy = self.copy(owner, h, to, index)
        copy.start()
        self.sent.append(copy)

    def arrived(self, owner, h, index):
        self.copy(owner, h, self.right, index).wait_recv()

    def start(self):
        self.send(self.mine, 0, self.right, 0)
        self.send(self.mine, 1, self.left, 1)
        self.send(self.mine, 1, self.right, 2)
        self.send(self.mine, 0, self.left, 3)

    def forward(self):
        self.arrived(self.right, 0, 0)
        self.send(self.right, 0, self.left, 5)
        self.arrived(self.left, 1, 1)
        self.send(self.left, 1, self.right, 4)

    def finish(self):
        self.arrived(self.right, 1, 2)
        self.arrived(self.left, 0, 3)
        self.arrived(self.far, 1, 4)
        self.arrived(self.far, 0, 5)

    def drain(self):
        for copy in self.sent:
            copy.wait_send()


def kernel(
    tok_hbm, gain_hbm, gate_hbm, up_hbm, down_hbm, ids_hbm, rw_hbm, out_ref,
    tok, gain, ids, rw,
    pbuf, gub, dnb, dnf, xb, hb, ob, rb, mixer,
    in_sem, disp_send, disp_recv, ret_send, ret_recv, ring_send, ring_recv,
):
    ep = lax.axis_index("ep")
    tp = lax.axis_index("tp")
    z, c = ep // 2, ep % 2
    (ay, by), (ax, bx) = bits(tp // Q), bits(tp % Q)
    side_a, side_b = ay * 2 + ax, by * 2 + bx
    quarter_of, column_of = (side_a, side_b), (side_b, side_a)
    quarter = side_a + c * (side_b - side_a)
    column = side_b + c * (side_a - side_b)

    barrier = pltpu.get_barrier_semaphore()

    def greet(device):
        pl.semaphore_signal(barrier, inc=1, device_id=device, device_id_type=MESH)

    def with_column(to):
        return (ep, place(c, to, column))

    def with_quarter(to):
        return (ep, place(c, quarter, to))

    for m in (2, 1, 3, 0):
        z_from = (z - (m * Q + quarter) + NZ) % NZ
        for cs in range(2):
            for qs in range(Q):
                device = (z_from * 2 + cs, place(c, qs, column))
                if m == 0 and qs == 0:
                    @pl.when(jnp.logical_not(jnp.logical_and(quarter == 0, c == cs)))
                    def _():
                        greet(device)
                else:
                    greet(device)

    loads = []
    for i, (src, dst) in enumerate(
        ((ids_hbm, ids), (tok_hbm, tok), (gate_hbm.at[0], gub.at[quarter, pl.ds(0, HALF)]),
         (up_hbm.at[0], gub.at[quarter, pl.ds(HALF, HALF)]), (down_hbm.at[0], dnb.at[quarter]),
         (gain_hbm, gain), (rw_hbm, rw))
    ):
        load = pltpu.make_async_copy(src, dst, in_sem.at[i])
        load.start()
        loads.append(load)

    sems = (ring_send, ring_recv)
    gu = Gather(lambda o, h: gub.at[o, pl.ds(h * HALF, HALF)], quarter, with_column, sems, 0)
    dn = Gather(lambda o, h: dnb.at[o, pl.ds(h * 32, 32)], quarter, with_column, sems, 6)
    x_parts, h_parts = [], []
    for i in range(N_PART):
        span = pl.ds(i * PACKED, PACKED)
        x_parts.append(Gather(
            lambda o, h, span=span: xb.at[o, pl.ds(h * 2, 2), span], column, with_quarter, sems, 12 + 12 * i
        ))
        h_parts.append(Gather(
            lambda o, h, i=i: hb.at[i, o, h], column, with_quarter, sems, 18 + 12 * i
        ))
    for gather in (gu, x_parts[0]):
        greet(gather.device(gather.right))
        greet(gather.device(gather.left))

    loads[0].wait()
    experts = iota((EXPERTS, TOK), 0)
    named = [ids[k : k + 1, :] == experts for k in range(TOPK)]
    member = named[0] | named[1] | named[2] | named[3]
    earlier = jnp.where(iota((TOK, TOK), 0) < iota((TOK, TOK), 1), 1.0, 0.0).astype(BF16)
    slot = dot(jnp.where(member, 1.0, 0.0).astype(BF16), earlier)
    code = jnp.where(member, slot, -1.0).astype(BF16)
    expand = jnp.where(iota((512, EXPERTS), 0) // 16 == iota((512, EXPERTS), 1), 1.0, 0.0).astype(BF16)
    code_wide = dot(expand, code)
    slot_of_row = (iota((512, TOK), 0) % 16).astype(F32)
    pick_low = jnp.where(code_wide == slot_of_row, 1.0, 0.0)
    pick_high = jnp.where(code_wide == slot_of_row + 16.0, 1.0, 0.0)

    loads[1].wait()
    token_low = dot_columns(tok[...], placed(0)).astype(BF16)
    token_high = dot_columns(tok[...], placed(HALF)).astype(BF16)
    packed = dot(pick_low.astype(BF16), token_low) + dot(pick_high.astype(BF16), token_high)
    pbuf[...] = packed.astype(BF16)

    pl.semaphore_wait(barrier, 2 * NZ + 4 - jnp.where(quarter == 0, 1, 0))

    sends = []
    for dz in Z_ORDER:
        m = dz // Q
        for ce in range(2):
            e = ((z + dz) % NZ) * 2 + ce
            copy = pltpu.make_async_remote_copy(
                src_ref=pbuf.at[tile(e * 16)],
                dst_ref=xb.at[column_of[ce], quarter_of[ce], tile(rows_at(m, c))],
                send_sem=disp_send.at[dz * 2 + ce],
                recv_sem=disp_recv.at[(m * 2 + c) * Q + quarter_of[ce]],
                device_id=(e, place(ce, dz % Q, column_of[ce])),
                device_id_type=MESH,
            )
            if dz == 0:
                own = jnp.logical_and(quarter == 0, c == ce)

                @pl.when(jnp.logical_not(own))
                def _():
                    copy.start()

                @pl.when(own)
                def _():
                    xb[column, 0, tile(rows_at(0, c)), :] = pbuf[tile(e * 16), :]
                sends.append((copy, own))
            else:
                copy.start()
                sends.append((copy, None))

    for load in loads[2:5]:
        load.wait()
    gu.start()
    dn.start()

    loads[5].wait()
    loads[6].wait()
    weight = jnp.zeros((EXPERTS, TOK), F32)
    for k in range(TOPK):
        weight = weight + jnp.where(named[k], rw[k : k + 1, :], 0.0)
    for i in range(3):
        piece = weight.astype(BF16)
        weight = weight - piece.astype(F32)
        wide = dot(expand, piece)
        mixer[:, i * 128 : i * 128 + 128] = (wide * pick_low).astype(BF16)
        mixer[:, 384 + i * 128 : 512 + i * 128] = (wide * pick_high).astype(BF16)

    gu.forward()

    def await_dispatch(part):
        for m in PARTS[part]:
            for cs in range(2):
                for qs in range(Q):
                    arrived = pltpu.make_async_remote_copy(
                        src_ref=pbuf.at[tile(0)],
                        dst_ref=xb.at[column, qs, tile(rows_at(m, cs))],
                        send_sem=disp_send.at[0],
                        recv_sem=disp_recv.at[(m * 2 + cs) * Q + qs],
                        device_id=(ep, tp),
                        device_id_type=MESH,
                    )
                    if m == 0 and qs == 0:
                        @pl.when(jnp.logical_not(jnp.logical_and(quarter == 0, c == cs)))
                        def _():
                            arrived.wait_recv()
                    else:
                        arrived.wait_recv()

    def slice_at(s, part):
        (ty, uy), (tx, ux) = bits(s // Q), bits(s % Q)
        t, u = ty * 2 + tx, uy * 2 + ux
        return xb[u + c * (t - u), t + c * (u - t), part * PACKED : (part + 1) * PACKED].astype(F32)

    def make_hidden(part):
        groups = []
        square = jnp.zeros((2 * PACKED, 128), F32)
        for g in range(8):
            low, high = swap(slice_at(2 * g, part), slice_at(2 * g + 1, part))
            both = jnp.concatenate([low, high], axis=0)
            square = square + both * both
            groups.append(both)
        inverse = lax.rsqrt(jnp.sum(square, axis=1, keepdims=True) / D + EPSILON)
        rows = jnp.concatenate(
            [(groups[g] * inverse * gain[g : g + 1, :]).astype(BF16) for g in range(8)], axis=1
        )
        for p in range(2):
            both = dot_rows(rows, jnp.concatenate([gub[2 * p], gub[2 * p + 1]], axis=0))
            gate_pre, up_pre = swap(both[:, :128], both[:, 128:])
            gate_pre = jnp.minimum(gate_pre, LIMIT)
            up_pre = jnp.clip(up_pre, -LIMIT, LIMIT)
            hidden = (up_pre + 1.0) * gate_pre * jax.nn.sigmoid(ALPHA * gate_pre)
            hb[part, column, p] = hidden.astype(BF16)

    def order_down(k):
        low = iota((HALF, 128), 1) < HALF
        for n in range(Q):
            for o in range(Q):
                for p in range(2):
                    sides = []
                    for h in range(2):
                        s = place(k, 2 * p + h, o)
                        v = dnb[n, :, s // 2 * 128 : s // 2 * 128 + 128].astype(F32)
                        sides.append(v if s % 2 == h else pltpu.roll(v, HALF, 1))
                    at = (o * 2 + p) * 128
                    dnf[n * HALF : n * HALF + HALF, at : at + 128] = jnp.where(low, *sides).astype(BF16)

    def make_result(part):
        hidden_all = jnp.concatenate([hb[part, k // 2, k % 2] for k in range(8)], axis=1)
        result = dot_rows(hidden_all, dnf[...])
        at = part * PACKED
        for n in range(2):
            cols = result[:, n * 128 : n * 128 + 128]
            pair = swap(cols[:PACKED], cols[PACKED:])
            ob[2 * n, at : at + PACKED], ob[2 * n + 1, at : at + PACKED] = [v.astype(BF16) for v in pair]

    def send_back(part):
        for m in PARTS[part]:
            z_to = (z - (m * Q + quarter) + NZ) % NZ
            for cs in range(2):
                for qs in range(Q):
                    copy = pltpu.make_async_remote_copy(
                        src_ref=ob.at[qs, tile(rows_at(m, cs))],
                        dst_ref=rb.at[tile(ep * 16)],
                        send_sem=ret_send.at[(m * 2 + cs) * Q + qs],
                        recv_sem=ret_recv.at[ep],
                        device_id=(z_to * 2 + cs, place(c, qs, column)),
                        device_id_type=MESH,
                    )
                    if m == 0 and qs == 0:
                        own = jnp.logical_and(quarter == 0, c == cs)

                        @pl.when(jnp.logical_not(own))
                        def _():
                            copy.start()

                        @pl.when(own)
                        def _():
                            rb[tile(ep * 16), :] = ob[0, tile(rows_at(0, cs)), :]
                        sends.append((copy, own))
                    else:
                        copy.start()
                        sends.append((copy, None))

    near, far = 0, 1
    await_dispatch(near)
    x_parts[near].start()
    dn.forward()
    x_parts[near].forward()
    x_parts[near].finish()
    gu.finish()
    make_hidden(near)
    h_parts[near].start()
    await_dispatch(far)
    x_parts[far].start()
    h_parts[near].forward()
    dn.finish()
    for k in range(2):
        @pl.when(c == k)
        def _():
            order_down(k)
    x_parts[far].forward()
    x_parts[far].finish()
    make_hidden(far)
    h_parts[far].start()
    h_parts[near].finish()
    make_result(near)
    send_back(near)
    h_parts[far].forward()
    h_parts[far].finish()
    make_result(far)
    send_back(far)

    for dz in range(NZ):
        for ce in range(2):
            e = ((z + dz) % NZ) * 2 + ce
            arrived = pltpu.make_async_remote_copy(
                src_ref=ob.at[0, tile(0)],
                dst_ref=rb.at[tile(e * 16)],
                send_sem=ret_send.at[0],
                recv_sem=ret_recv.at[e],
                device_id=(ep, tp),
                device_id_type=MESH,
            )
            if dz == 0:
                @pl.when(jnp.logical_not(jnp.logical_and(quarter_of[ce] == 0, c == ce)))
                def _():
                    arrived.wait_recv()
            else:
                arrived.wait_recv()

    mixed = dot_columns(rb[...], mixer[...])
    combined = mixed[0:HALF, 0:128] + mixed[HALF:128, 384:512]
    for i in range(1, 3):
        combined = combined + mixed[0:HALF, i * 128 : i * 128 + 128]
        combined = combined + mixed[HALF:128, 384 + i * 128 : 512 + i * 128]
    out_ref[...] = combined.astype(BF16)

    for copy, own in sends:
        if own is None:
            copy.wait_send()
        else:
            @pl.when(jnp.logical_not(own))
            def _():
                copy.wait_send()
    for gather in [gu, dn] + x_parts + h_parts:
        gather.drain()


def body(tokens, norm_gain, gate_weight, up_weight, down_weight, expert_ids, route_weight):
    turned = (0, 2, 1)
    return pl.pallas_call(
        kernel,
        out_shape=jax.ShapeDtypeStruct((HALF, TOK), BF16),
        in_specs=[pl.BlockSpec(memory_space=pl.ANY)] * 7,
        out_specs=pl.BlockSpec(memory_space=pltpu.VMEM),
        scratch_shapes=[
            pltpu.VMEM((HALF, TOK), BF16),
            pltpu.VMEM((8, 128), F32),
            pltpu.VMEM((TOPK, TOK), jnp.int32),
            pltpu.VMEM((TOPK, TOK), F32),
            pltpu.VMEM((512, 128), BF16),
            pltpu.VMEM((Q, 128, D), BF16),
            pltpu.VMEM((Q, HALF, D), BF16),
            pltpu.VMEM((256, D), BF16),
            pltpu.VMEM((Q, Q, 128, 128), BF16),
            pltpu.VMEM((N_PART, Q, 2, 2 * PACKED, 128), BF16),
            pltpu.VMEM((Q, 128, 128), BF16),
            pltpu.VMEM((512, 128), BF16),
            pltpu.VMEM((512, 768), BF16),
            pltpu.SemaphoreType.DMA((7,)),
            pltpu.SemaphoreType.DMA((32,)),
            pltpu.SemaphoreType.DMA((32,)),
            pltpu.SemaphoreType.DMA((32,)),
            pltpu.SemaphoreType.DMA((32,)),
            pltpu.SemaphoreType.DMA((12 + 12 * N_PART,)),
            pltpu.SemaphoreType.DMA((12 + 12 * N_PART,)),
        ],
        compiler_params=pltpu.CompilerParams(collective_id=0, has_side_effects=True),
    )(
        tokens.T, norm_gain.reshape(8, 128), gate_weight.transpose(turned), up_weight.transpose(turned),
        down_weight.transpose(turned), expert_ids.T, route_weight.T,
    ).T


def solution(mesh):
    in_specs = (
        P("ep", "tp"),
        P(),
        P("ep", None, "tp"),
        P("ep", None, "tp"),
        P("ep", None, "tp"),
        P("ep", None),
        P("ep", None),
    )
    return jax.shard_map(body, mesh=mesh, in_specs=in_specs, out_specs=P("ep", "tp"), check_vma=False)
```

```python
import jax
import jax.numpy as jnp
from jax import lax
from jax.experimental import pallas as pl
from jax.experimental.pallas import tpu as pltpu
from jax.sharding import PartitionSpec as P

MESH = pl.DeviceIdType.MESH
F32 = jnp.float32
BF16 = jnp.bfloat16

EPSILON = 1e-06
ALPHA = 1.702
LIMIT = 7.0

NZ = 16
Q = 4
D = 1024
TOK = 128
EXPERTS = 32
TOPK = 4
HALF = 64
Z_ORDER = (8, 7, 9, 6, 10, 5, 11, 4, 12, 3, 13, 2, 14, 1, 15, 0)
PARTS = ((2, 1), (3, 0))
M_AT = {m: i for i, m in enumerate(m for part in PARTS for m in part)}
N_PART = len(PARTS)
PACKED = 128 // N_PART


def iota(shape, dim):
    return lax.broadcasted_iota(jnp.int32, shape, dim)


def dot(a, b):
    return jnp.dot(a, b, preferred_element_type=F32)


def dot_rows(a, b):
    return lax.dot_general(a, b, (((1,), (1,)), ((), ())), preferred_element_type=F32)


def dot_columns(a, b):
    return lax.dot_general(a, b, (((0,), (0,)), ((), ())), preferred_element_type=F32)


def placed(offset):
    return jnp.where(iota((HALF, 128), 1) == iota((HALF, 128), 0) + offset, 1.0, 0.0).astype(BF16)


def swap(a, b):
    low = iota(a.shape, 1) < HALF
    return jnp.where(low, a, pltpu.roll(b, HALF, 1)), jnp.where(low, pltpu.roll(a, HALF, 1), b)


def bits(v):
    return v // 2, ((v + 1) % Q) // 2


def gray(a, b):
    return 3 * a + b - 2 * a * b


def place(k, quarter, column):
    if isinstance(k, int):
        a, b = (quarter, column) if k == 0 else (column, quarter)
    else:
        a = quarter + k * (column - quarter)
        b = column + k * (quarter - column)
    return gray(a // 2, b // 2) * Q + gray(a % 2, b % 2)


def rows_at(m, core):
    return (M_AT[m] * 2 + core) * 16


def tile(start):
    return pl.ds(start if isinstance(start, int) else pl.multiple_of(start, 16), 16)


class Gather:
    def __init__(self, view, mine, device, sems, base, direct=False):
        self.direct = direct
        self.view, self.device, self.base = view, device, base
        self.send_sems, self.recv_sems = sems
        self.mine = mine
        self.right = mine + 1 - 2 * (mine % 2)
        self.left = mine + 2 - 4 * (mine // 2)
        self.far = 3 - mine
        self.sent = []

    def copy(self, owner, h, to, index):
        return pltpu.make_async_remote_copy(
            src_ref=self.view(owner, h),
            dst_ref=self.view(owner, h),
            send_sem=self.send_sems.at[self.base + index],
            recv_sem=self.recv_sems.at[self.base + index],
            device_id=self.device(to),
            device_id_type=MESH,
        )

    def send(self, owner, h, to, index):
        copy = self.copy(owner, h, to, index)
        copy.start()
        self.sent.append(copy)

    def arrived(self, owner, h, index):
        self.copy(owner, h, self.right, index).wait_recv()

    def start(self):
        self.send(self.mine, 0, self.right, 0)
        self.send(self.mine, 1, self.left, 1)
        self.send(self.mine, 1, self.right, 2)
        self.send(self.mine, 0, self.left, 3)
        if self.direct:
            self.send(self.mine, 1, self.far, 4)
            self.send(self.mine, 0, self.far, 5)

    def forward(self):
        self.arrived(self.right, 0, 0)
        self.send(self.right, 0, self.left, 5)
        self.arrived(self.left, 1, 1)
        self.send(self.left, 1, self.right, 4)

    def finish(self):
        if self.direct:
            self.arrived(self.right, 0, 0)
            self.arrived(self.left, 1, 1)
        self.arrived(self.right, 1, 2)
        self.arrived(self.left, 0, 3)
        self.arrived(self.far, 1, 4)
        self.arrived(self.far, 0, 5)

    def drain(self):
        for copy in self.sent:
            copy.wait_send()


def kernel(
    tok_hbm, gain_hbm, gate_hbm, up_hbm, down_hbm, ids_hbm, rw_hbm, out_ref,
    tok, gain, ids, rw,
    pbuf, gub, dnb, dnf, xb, hb, ob, rb, mixer,
    in_sem, disp_send, disp_recv, ret_send, ret_recv, ring_send, ring_recv,
):
    ep = lax.axis_index("ep")
    tp = lax.axis_index("tp")
    z, c = ep // 2, ep % 2
    (ay, by), (ax, bx) = bits(tp // Q), bits(tp % Q)
    side_a, side_b = ay * 2 + ax, by * 2 + bx
    quarter_of, column_of = (side_a, side_b), (side_b, side_a)
    quarter = side_a + c * (side_b - side_a)
    column = side_b + c * (side_a - side_b)

    loads = []
    for i, (src, dst) in enumerate(
        ((ids_hbm, ids), (tok_hbm, tok), (gate_hbm.at[0], gub.at[quarter, pl.ds(0, HALF)]),
         (up_hbm.at[0], gub.at[quarter, pl.ds(HALF, HALF)]), (down_hbm.at[0], dnb.at[quarter]),
         (gain_hbm, gain), (rw_hbm, rw))
    ):
        load = pltpu.make_async_copy(src, dst, in_sem.at[i])
        load.start()
        loads.append(load)

    barrier = pltpu.get_barrier_semaphore()

    def greet(device):
        pl.semaphore_signal(barrier, inc=1, device_id=device, device_id_type=MESH)

    def with_column(to):
        return (ep, place(c, to, column))

    def with_quarter(to):
        return (ep, place(c, quarter, to))

    for m in (2, 1, 3, 0):
        z_from = (z - (m * Q + quarter) + NZ) % NZ
        for cs in range(2):
            for qs in range(Q):
                device = (z_from * 2 + cs, place(c, qs, column))
                if m == 0 and qs == 0:
                    @pl.when(jnp.logical_not(jnp.logical_and(quarter == 0, c == cs)))
                    def _():
                        greet(device)
                else:
                    greet(device)

    sems = (ring_send, ring_recv)
    gu = Gather(lambda o, h: gub.at[o, pl.ds(h * HALF, HALF)], quarter, with_column, sems, 0)
    dn = Gather(lambda o, h: dnb.at[o, pl.ds(h * 32, 32)], quarter, with_column, sems, 6)
    x_parts, h_parts = [], []
    for i in range(N_PART):
        span = pl.ds(i * PACKED, PACKED)
        x_parts.append(Gather(
            lambda o, h, span=span: xb.at[o, pl.ds(h * 2, 2), span], column, with_quarter, sems, 12 + 12 * i, True
        ))
        h_parts.append(Gather(
            lambda o, h, i=i: hb.at[i, o, h], column, with_quarter, sems, 18 + 12 * i, True
        ))
    for gather in (gu, x_parts[0]):
        greet(gather.device(gather.right))
        greet(gather.device(gather.left))
    greet(x_parts[0].device(x_parts[0].far))

    loads[0].wait()
    experts = iota((EXPERTS, TOK), 0)
    named = [ids[k : k + 1, :] == experts for k in range(TOPK)]
    member = named[0] | named[1] | named[2] | named[3]
    earlier = jnp.where(iota((TOK, TOK), 0) < iota((TOK, TOK), 1), 1.0, 0.0).astype(BF16)
    slot = dot(jnp.where(member, 1.0, 0.0).astype(BF16), earlier)
    code = jnp.where(member, slot, -1.0).astype(BF16)
    expand = jnp.where(iota((512, EXPERTS), 0) // 16 == iota((512, EXPERTS), 1), 1.0, 0.0).astype(BF16)
    code_wide = dot(expand, code)
    slot_of_row = (iota((512, TOK), 0) % 16).astype(F32)
    pick_low = jnp.where(code_wide == slot_of_row, 1.0, 0.0)
    pick_high = jnp.where(code_wide == slot_of_row + 16.0, 1.0, 0.0)

    loads[1].wait()
    token_low = dot_columns(tok[...], placed(0)).astype(BF16)
    token_high = dot_columns(tok[...], placed(HALF)).astype(BF16)
    packed = dot(pick_low.astype(BF16), token_low) + dot(pick_high.astype(BF16), token_high)
    pbuf[...] = packed.astype(BF16)

    pl.semaphore_wait(barrier, 2 * NZ + 5 - jnp.where(quarter == 0, 1, 0))

    sends = []
    for dz in Z_ORDER:
        m = dz // Q
        for ce in range(2):
            e = ((z + dz) % NZ) * 2 + ce
            copy = pltpu.make_async_remote_copy(
                src_ref=pbuf.at[tile(e * 16)],
                dst_ref=xb.at[column_of[ce], quarter_of[ce], tile(rows_at(m, c))],
                send_sem=disp_send.at[dz * 2 + ce],
                recv_sem=disp_recv.at[(m * 2 + c) * Q + quarter_of[ce]],
                device_id=(e, place(ce, dz % Q, column_of[ce])),
                device_id_type=MESH,
            )
            if dz == 0:
                own = jnp.logical_and(quarter == 0, c == ce)

                @pl.when(jnp.logical_not(own))
                def _():
                    copy.start()

                @pl.when(own)
                def _():
                    xb[column, 0, tile(rows_at(0, c)), :] = pbuf[tile(e * 16), :]
                sends.append((copy, own))
            else:
                copy.start()
                sends.append((copy, None))

    for load in loads[2:5]:
        load.wait()
    gu.start()
    dn.start()

    loads[5].wait()
    loads[6].wait()
    weight = jnp.zeros((EXPERTS, TOK), F32)
    for k in range(TOPK):
        weight = weight + jnp.where(named[k], rw[k : k + 1, :], 0.0)
    for i in range(3):
        piece = weight.astype(BF16)
        weight = weight - piece.astype(F32)
        wide = dot(expand, piece)
        mixer[:, i * 128 : i * 128 + 128] = (wide * pick_low).astype(BF16)
        mixer[:, 384 + i * 128 : 512 + i * 128] = (wide * pick_high).astype(BF16)

    gu.forward()
    dn.forward()

    def await_dispatch(part):
        for m in PARTS[part]:
            for cs in range(2):
                for qs in range(Q):
                    arrived = pltpu.make_async_remote_copy(
                        src_ref=pbuf.at[tile(0)],
                        dst_ref=xb.at[column, qs, tile(rows_at(m, cs))],
                        send_sem=disp_send.at[0],
                        recv_sem=disp_recv.at[(m * 2 + cs) * Q + qs],
                        device_id=(ep, tp),
                        device_id_type=MESH,
                    )
                    if m == 0 and qs == 0:
                        @pl.when(jnp.logical_not(jnp.logical_and(quarter == 0, c == cs)))
                        def _():
                            arrived.wait_recv()
                    else:
                        arrived.wait_recv()

    def slice_at(s, part):
        (ty, uy), (tx, ux) = bits(s // Q), bits(s % Q)
        t, u = ty * 2 + tx, uy * 2 + ux
        return xb[u + c * (t - u), t + c * (u - t), part * PACKED : (part + 1) * PACKED].astype(F32)

    def make_hidden(part):
        groups = []
        square = jnp.zeros((2 * PACKED, 128), F32)
        for g in range(8):
            low, high = swap(slice_at(2 * g, part), slice_at(2 * g + 1, part))
            both = jnp.concatenate([low, high], axis=0)
            square = square + both * both
            groups.append(both)
        inverse = lax.rsqrt(jnp.sum(square, axis=1, keepdims=True) / D + EPSILON)
        rows = jnp.concatenate(
            [(groups[g] * inverse * gain[g : g + 1, :]).astype(BF16) for g in range(8)], axis=1
        )
        for p in range(2):
            both = dot_rows(rows, jnp.concatenate([gub[2 * p], gub[2 * p + 1]], axis=0))
            gate_pre, up_pre = swap(both[:, :128], both[:, 128:])
            gate_pre = jnp.minimum(gate_pre, LIMIT)
            up_pre = jnp.clip(up_pre, -LIMIT, LIMIT)
            hidden = (up_pre + 1.0) * gate_pre * jax.nn.sigmoid(ALPHA * gate_pre)
            hb[part, column, p] = hidden.astype(BF16)

    def order_down(k):
        low = iota((HALF, 128), 1) < HALF
        for n in range(Q):
            for o in range(Q):
                for p in range(2):
                    sides = []
                    for h in range(2):
                        s = place(k, 2 * p + h, o)
                        v = dnb[n, :, s // 2 * 128 : s // 2 * 128 + 128].astype(F32)
                        sides.append(v if s % 2 == h else pltpu.roll(v, HALF, 1))
                    at = (o * 2 + p) * 128
                    dnf[n * HALF : n * HALF + HALF, at : at + 128] = jnp.where(low, *sides).astype(BF16)

    def make_result(part):
        hidden_all = jnp.concatenate([hb[part, k // 2, k % 2] for k in range(8)], axis=1)
        result = dot_rows(hidden_all, dnf[...])
        at = part * PACKED
        for n in range(2):
            cols = result[:, n * 128 : n * 128 + 128]
            pair = swap(cols[:PACKED], cols[PACKED:])
            ob[2 * n, at : at + PACKED], ob[2 * n + 1, at : at + PACKED] = [v.astype(BF16) for v in pair]

    def send_back(part):
        for m in PARTS[part]:
            z_to = (z - (m * Q + quarter) + NZ) % NZ
            for cs in range(2):
                for qs in range(Q):
                    copy = pltpu.make_async_remote_copy(
                        src_ref=ob.at[qs, tile(rows_at(m, cs))],
                        dst_ref=rb.at[tile(ep * 16)],
                        send_sem=ret_send.at[(m * 2 + cs) * Q + qs],
                        recv_sem=ret_recv.at[ep],
                        device_id=(z_to * 2 + cs, place(c, qs, column)),
                        device_id_type=MESH,
                    )
                    if m == 0 and qs == 0:
                        own = jnp.logical_and(quarter == 0, c == cs)

                        @pl.when(jnp.logical_not(own))
                        def _():
                            copy.start()

                        @pl.when(own)
                        def _():
                            rb[tile(ep * 16), :] = ob[0, tile(rows_at(0, cs)), :]
                        sends.append((copy, own))
                    else:
                        copy.start()
                        sends.append((copy, None))

    far, near = 0, 1
    await_dispatch(far)
    x_parts[far].start()
    await_dispatch(near)
    x_parts[near].start()
    x_parts[far].finish()
    gu.finish()
    make_hidden(far)
    h_parts[far].start()
    dn.finish()
    for k in range(2):
        @pl.when(c == k)
        def _():
            order_down(k)
    x_parts[near].finish()
    make_hidden(near)
    h_parts[near].start()
    h_parts[far].finish()
    make_result(far)
    send_back(far)
    h_parts[near].finish()
    make_result(near)
    send_back(near)

    for dz in range(NZ):
        for ce in range(2):
            e = ((z + dz) % NZ) * 2 + ce
            arrived = pltpu.make_async_remote_copy(
                src_ref=ob.at[0, tile(0)],
                dst_ref=rb.at[tile(e * 16)],
                send_sem=ret_send.at[0],
                recv_sem=ret_recv.at[e],
                device_id=(ep, tp),
                device_id_type=MESH,
            )
            if dz == 0:
                @pl.when(jnp.logical_not(jnp.logical_and(quarter_of[ce] == 0, c == ce)))
                def _():
                    arrived.wait_recv()
            else:
                arrived.wait_recv()

    mixed = dot_columns(rb[...], mixer[...])
    combined = mixed[0:HALF, 0:128] + mixed[HALF:128, 384:512]
    for i in range(1, 3):
        combined = combined + mixed[0:HALF, i * 128 : i * 128 + 128]
        combined = combined + mixed[HALF:128, 384 + i * 128 : 512 + i * 128]
    out_ref[...] = combined.astype(BF16)

    for copy, own in sends:
        if own is None:
            copy.wait_send()
        else:
            @pl.when(jnp.logical_not(own))
            def _():
                copy.wait_send()
    for gather in [gu, dn] + x_parts + h_parts:
        gather.drain()


def body(tokens, norm_gain, gate_weight, up_weight, down_weight, expert_ids, route_weight):
    turned = (0, 2, 1)
    return pl.pallas_call(
        kernel,
        out_shape=jax.ShapeDtypeStruct((HALF, TOK), BF16),
        in_specs=[pl.BlockSpec(memory_space=pl.ANY)] * 7,
        out_specs=pl.BlockSpec(memory_space=pltpu.VMEM),
        scratch_shapes=[
            pltpu.VMEM((HALF, TOK), BF16),
            pltpu.VMEM((8, 128), F32),
            pltpu.VMEM((TOPK, TOK), jnp.int32),
            pltpu.VMEM((TOPK, TOK), F32),
            pltpu.VMEM((512, 128), BF16),
            pltpu.VMEM((Q, 128, D), BF16),
            pltpu.VMEM((Q, HALF, D), BF16),
            pltpu.VMEM((256, D), BF16),
            pltpu.VMEM((Q, Q, 128, 128), BF16),
            pltpu.VMEM((N_PART, Q, 2, 2 * PACKED, 128), BF16),
            pltpu.VMEM((Q, 128, 128), BF16),
            pltpu.VMEM((512, 128), BF16),
            pltpu.VMEM((512, 768), BF16),
            pltpu.SemaphoreType.DMA((7,)),
            pltpu.SemaphoreType.DMA((32,)),
            pltpu.SemaphoreType.DMA((32,)),
            pltpu.SemaphoreType.DMA((32,)),
            pltpu.SemaphoreType.DMA((32,)),
            pltpu.SemaphoreType.DMA((12 + 12 * N_PART,)),
            pltpu.SemaphoreType.DMA((12 + 12 * N_PART,)),
        ],
        compiler_params=pltpu.CompilerParams(collective_id=0, has_side_effects=True),
    )(
        tokens.T, norm_gain.reshape(8, 128), gate_weight.transpose(turned), up_weight.transpose(turned),
        down_weight.transpose(turned), expert_ids.T, route_weight.T,
    ).T


def solution(mesh):
    in_specs = (
        P("ep", "tp"),
        P(),
        P("ep", None, "tp"),
        P("ep", None, "tp"),
        P("ep", None, "tp"),
        P("ep", None),
        P("ep", None),
    )
    return jax.shard_map(body, mesh=mesh, in_specs=in_specs, out_specs=P("ep", "tp"), check_vma=False)
```

```python
import jax
import jax.numpy as jnp
from jax import lax
from jax.experimental import pallas as pl
from jax.experimental.pallas import tpu as pltpu
from jax.sharding import PartitionSpec as P

MESH = pl.DeviceIdType.MESH
F32 = jnp.float32
BF16 = jnp.bfloat16

EPSILON = 1e-06
ALPHA = 1.702
LIMIT = 7.0

NZ = 16
Q = 4
D = 1024
TOK = 128
EXPERTS = 32
TOPK = 4
HALF = 64
Z_ORDER = (8, 7, 9, 6, 10, 5, 11, 4, 12, 3, 13, 2, 14, 1, 15, 0)
PARTS = ((0,), (1,), (2, 3))
N_PART = len(PARTS)


def iota(shape, dim):
    return lax.broadcasted_iota(jnp.int32, shape, dim)


def dot(a, b):
    return jnp.dot(a, b, preferred_element_type=F32)


def dot_rows(a, b):
    return lax.dot_general(a, b, (((1,), (1,)), ((), ())), preferred_element_type=F32)


def dot_columns(a, b):
    return lax.dot_general(a, b, (((0,), (0,)), ((), ())), preferred_element_type=F32)


def placed(offset):
    return jnp.where(iota((HALF, 128), 1) == iota((HALF, 128), 0) + offset, 1.0, 0.0).astype(BF16)


def swap(a, b):
    low = iota(a.shape, 1) < HALF
    return jnp.where(low, a, pltpu.roll(b, HALF, 1)), jnp.where(low, pltpu.roll(a, HALF, 1), b)


def bits(v):
    return v // 2, ((v + 1) % Q) // 2


def gray(a, b):
    return 3 * a + b - 2 * a * b


def place(k, quarter, column):
    if isinstance(k, int):
        a, b = (column, quarter) if k == 0 else (quarter, column)
    else:
        a = column + k * (quarter - column)
        b = quarter + k * (column - quarter)
    return gray(a // 2, b // 2) * Q + gray(a % 2, b % 2)


def rows_at(j, core):
    return (j * 2 + core) * 16


def tile(start):
    return pl.ds(start if isinstance(start, int) else pl.multiple_of(start, 16), 16)


class Gather:
    def __init__(self, view, mine, device, sems, base):
        self.view, self.device, self.base = view, device, base
        self.send_sems, self.recv_sems = sems
        self.mine = mine
        self.right = mine + 1 - 2 * (mine % 2)
        self.left = mine + 2 - 4 * (mine // 2)
        self.far = 3 - mine
        self.sent = []

    def copy(self, owner, h, to, index):
        return pltpu.make_async_remote_copy(
            src_ref=self.view(owner, h),
            dst_ref=self.view(owner, h),
            send_sem=self.send_sems.at[self.base + index],
            recv_sem=self.recv_sems.at[self.base + index],
            device_id=self.device(to),
            device_id_type=MESH,
        )

    def send(self, owner, h, to, index):
        copy = self.copy(owner, h, to, index)
        copy.start()
        self.sent.append(copy)

    def arrived(self, owner, h, index):
        self.copy(owner, h, self.right, index).wait_recv()

    def start(self):
        self.send(self.mine, 0, self.right, 0)
        self.send(self.mine, 1, self.left, 1)
        self.send(self.mine, 1, self.right, 2)
        self.send(self.mine, 0, self.left, 3)

    def forward(self):
        self.arrived(self.right, 0, 0)
        self.send(self.right, 0, self.left, 5)
        self.arrived(self.left, 1, 1)
        self.send(self.left, 1, self.right, 4)

    def finish(self):
        self.arrived(self.right, 1, 2)
        self.arrived(self.left, 0, 3)
        self.arrived(self.far, 1, 4)
        self.arrived(self.far, 0, 5)

    def drain(self):
        for copy in self.sent:
            copy.wait_send()


class Exchange:
    def __init__(self, view, pieces, mine, device, sems, base):
        self.view, self.device, self.base = view, device, base
        self.pieces = pieces
        self.send_sems, self.recv_sems = sems
        self.mine = mine
        self.right = mine + 1 - 2 * (mine % 2)
        self.left = mine + 2 - 4 * (mine // 2)
        self.far = 3 - mine
        self.others = (self.far, self.right, self.left)
        self.sent = []

    def copy(self, owner, h, to, index):
        return pltpu.make_async_remote_copy(
            src_ref=self.view(owner, h),
            dst_ref=self.view(owner, h),
            send_sem=self.send_sems.at[self.base + 3 * h + index],
            recv_sem=self.recv_sems.at[self.base + 3 * h + index],
            device_id=self.device(to),
            device_id_type=MESH,
        )

    def send(self, h):
        for index, to in enumerate(self.others):
            copy = self.copy(self.mine, h, to, index)
            copy.start()
            self.sent.append(copy)

    def arrived(self, index):
        for h in range(self.pieces):
            self.copy(self.others[index], h, self.right, index).wait_recv()

    def finish(self):
        for index in (1, 2, 0):
            self.arrived(index)

    def drain(self):
        for copy in self.sent:
            copy.wait_send()


def kernel(
    tok_hbm, gain_hbm, gate_hbm, up_hbm, down_hbm, ids_hbm, rw_hbm, out_ref,
    tok, gain, ids, rw,
    pbuf, gub, dnb, dnf, xb, hb, ob, rb, mixer,
    in_sem, disp_send, disp_recv, ret_send, ret_recv, ring_send, ring_recv,
):
    ep = lax.axis_index("ep")
    tp = lax.axis_index("tp")
    z, c = ep // 2, ep % 2
    (ay, by), (ax, bx) = bits(tp // Q), bits(tp % Q)
    side_a, side_b = ay * 2 + ax, by * 2 + bx
    quarter_of, column_of = (side_b, side_a), (side_a, side_b)
    quarter = side_b + c * (side_a - side_b)
    column = side_a + c * (side_b - side_a)

    loads = []
    for i, (src, dst) in enumerate(
        ((ids_hbm, ids), (tok_hbm, tok), (gate_hbm.at[0], gub.at[quarter, pl.ds(0, HALF)]),
         (up_hbm.at[0], gub.at[quarter, pl.ds(HALF, HALF)]), (down_hbm.at[0], dnb.at[quarter]),
         (gain_hbm, gain), (rw_hbm, rw))
    ):
        load = pltpu.make_async_copy(src, dst, in_sem.at[i])
        load.start()
        loads.append(load)

    barrier = pltpu.get_barrier_semaphore()

    def greet(device):
        pl.semaphore_signal(barrier, inc=1, device_id=device, device_id_type=MESH)

    def with_column(to):
        return (ep, place(c, to, column))

    def with_quarter(to):
        return (ep, place(c, quarter, to))

    z_low = (z - quarter + NZ) % Q

    def is_own(j, cs):
        return jnp.logical_and(jnp.logical_and(quarter == 0, c == cs), z // Q == j)

    for j in range(Q):
        z_from = j * Q + z_low
        for cs in range(2):
            for qs in range(Q):
                device = (z_from * 2 + cs, place(c, qs, column))
                if qs == 0:
                    @pl.when(jnp.logical_not(is_own(j, cs)))
                    def _():
                        greet(device)
                else:
                    greet(device)

    sems = (ring_send, ring_recv)
    gu = Gather(lambda o, h: gub.at[o, pl.ds(h * HALF, HALF)], quarter, with_column, sems, 0)
    dn = Gather(lambda o, h: dnb.at[o, pl.ds(h * 32, 32)], quarter, with_column, sems, 6)
    x_parts, h_parts = [], []
    for i, part in enumerate(PARTS):
        x_parts.append(Exchange(
            lambda o, h, first=part[0]: xb.at[o, :, pl.ds((first + h) * 32, 32)],
            len(part), column, with_quarter, sems, 12 + 12 * i,
        ))
        h_parts.append(Exchange(
            lambda o, h, part=part: hb.at[o, h, pl.ds(part[0] * 64, len(part) * 64)],
            2, column, with_quarter, sems, 18 + 12 * i,
        ))
    for gather in (gu, x_parts[0]):
        greet(gather.device(gather.right))
        greet(gather.device(gather.left))
    greet(x_parts[0].device(x_parts[0].far))

    loads[0].wait()
    experts = iota((EXPERTS, TOK), 0)
    named = [ids[k : k + 1, :] == experts for k in range(TOPK)]
    member = named[0] | named[1] | named[2] | named[3]
    earlier = jnp.where(iota((TOK, TOK), 0) < iota((TOK, TOK), 1), 1.0, 0.0).astype(BF16)
    slot = dot(jnp.where(member, 1.0, 0.0).astype(BF16), earlier)
    code = jnp.where(member, slot, -1.0).astype(BF16)
    expand = jnp.where(iota((512, EXPERTS), 0) // 16 == iota((512, EXPERTS), 1), 1.0, 0.0).astype(BF16)
    code_wide = dot(expand, code)
    slot_of_row = (iota((512, TOK), 0) % 16).astype(F32)
    pick_low = jnp.where(code_wide == slot_of_row, 1.0, 0.0)
    pick_high = jnp.where(code_wide == slot_of_row + 16.0, 1.0, 0.0)

    loads[1].wait()
    token_low = dot_columns(tok[...], placed(0)).astype(BF16)
    token_high = dot_columns(tok[...], placed(HALF)).astype(BF16)
    packed = dot(pick_low.astype(BF16), token_low) + dot(pick_high.astype(BF16), token_high)
    pbuf[...] = packed.astype(BF16)

    pl.semaphore_wait(barrier, 2 * NZ + 5 - jnp.where(quarter == 0, 1, 0))

    def is_mine(dz, ce):
        return jnp.logical_and(quarter == 0, c == ce) if dz == 0 else None

    def dispatch():
        for dz in Z_ORDER:
            for ce in range(2):
                e = ((z + dz) % NZ) * 2 + ce
                copy = pltpu.make_async_remote_copy(
                    src_ref=pbuf.at[tile(e * 16)],
                    dst_ref=xb.at[column_of[ce], quarter_of[ce], tile(rows_at(z // Q, c))],
                    send_sem=disp_send.at[dz * 2 + ce],
                    recv_sem=disp_recv.at[(z // Q * 2 + c) * Q + quarter_of[ce]],
                    device_id=(e, place(ce, dz % Q, column_of[ce])),
                    device_id_type=MESH,
                )
                if dz == 0:
                    @pl.when(jnp.logical_not(is_mine(dz, ce)))
                    def _():
                        copy.start()

                    @pl.when(is_mine(dz, ce))
                    def _():
                        xb[column, 0, tile(rows_at(z // Q, c)), :] = pbuf[tile(e * 16), :]
                else:
                    copy.start()

    sends = []
    for dz in Z_ORDER:
        for ce in range(2):
            sends.append((pltpu.make_async_remote_copy(
                src_ref=pbuf.at[tile(0)],
                dst_ref=pbuf.at[tile(0)],
                send_sem=disp_send.at[dz * 2 + ce],
                recv_sem=disp_recv.at[0],
                device_id=(ep, tp),
                device_id_type=MESH,
            ), is_mine(dz, ce)))

    dispatch()

    for load in loads[2:5]:
        load.wait()
    gu.start()
    dn.start()

    loads[5].wait()
    loads[6].wait()
    weight = jnp.zeros((EXPERTS, TOK), F32)
    for k in range(TOPK):
        weight = weight + jnp.where(named[k], rw[k : k + 1, :], 0.0)
    for i in range(3):
        piece = weight.astype(BF16)
        weight = weight - piece.astype(F32)
        wide = dot(expand, piece)
        mixer[:, i * 128 : i * 128 + 128] = (wide * pick_low).astype(BF16)
        mixer[:, 384 + i * 128 : 512 + i * 128] = (wide * pick_high).astype(BF16)

    gu.forward()
    dn.forward()

    def pass_rows(part):
        for h, j in enumerate(PARTS[part]):
            for cs in range(2):
                for qs in range(Q):
                    arrived = pltpu.make_async_remote_copy(
                        src_ref=pbuf.at[tile(0)],
                        dst_ref=xb.at[column, qs, tile(rows_at(j, cs))],
                        send_sem=disp_send.at[0],
                        recv_sem=disp_recv.at[(j * 2 + cs) * Q + qs],
                        device_id=(ep, tp),
                        device_id_type=MESH,
                    )
                    if qs == 0:
                        @pl.when(jnp.logical_not(is_own(j, cs)))
                        def _():
                            arrived.wait_recv()
                    else:
                        arrived.wait_recv()
            x_parts[part].send(h)

    def slice_at(s, part):
        (ty, uy), (tx, ux) = bits(s // Q), bits(s % Q)
        t, u = ty * 2 + tx, uy * 2 + ux
        first, last = PARTS[part][0] * 32, PARTS[part][-1] * 32 + 32
        return xb[t + c * (u - t), u + c * (t - u), first:last].astype(F32)

    def make_hidden(part):
        groups = []
        at, count = PARTS[part][0] * 64, len(PARTS[part]) * 64
        square = jnp.zeros((count, 128), F32)
        for g in range(8):
            low, high = swap(slice_at(2 * g, part), slice_at(2 * g + 1, part))
            both = jnp.concatenate([low, high], axis=0)
            square = square + both * both
            groups.append(both)
        inverse = lax.rsqrt(jnp.sum(square, axis=1, keepdims=True) / D + EPSILON)
        rows = jnp.concatenate(
            [(groups[g] * inverse * gain[g : g + 1, :]).astype(BF16) for g in range(8)], axis=1
        )
        for p in range(2):
            both = dot_rows(rows, jnp.concatenate([gub[2 * p], gub[2 * p + 1]], axis=0))
            gate_pre, up_pre = swap(both[:, :128], both[:, 128:])
            gate_pre = jnp.minimum(gate_pre, LIMIT)
            up_pre = jnp.clip(up_pre, -LIMIT, LIMIT)
            hidden = (up_pre + 1.0) * gate_pre * jax.nn.sigmoid(ALPHA * gate_pre)
            hb[column, p, at : at + count] = hidden.astype(BF16)
            h_parts[part].send(p)

    def order_down(k):
        low = iota((HALF, 128), 1) < HALF
        for n in range(Q):
            for o in range(Q):
                for p in range(2):
                    sides = []
                    for h in range(2):
                        s = place(k, 2 * p + h, o)
                        v = dnb[n, :, s // 2 * 128 : s // 2 * 128 + 128].astype(F32)
                        sides.append(v if s % 2 == h else pltpu.roll(v, HALF, 1))
                    dnf[o, n * HALF : n * HALF + HALF, p * 128 : p * 128 + 128] = jnp.where(low, *sides).astype(BF16)

    def make_result(part):
        exchange = h_parts[part]
        at, count = PARTS[part][0] * 32, len(PARTS[part]) * 32

        def term(owner):
            units = jnp.concatenate([hb[owner, p, 2 * at : 2 * at + 2 * count] for p in range(2)], axis=1)
            return dot_rows(units, dnf[owner])

        result = term(column)
        for index in (1, 2, 0):
            exchange.arrived(index)
            result = result + term(exchange.others[index])
        for n in range(2):
            cols = result[:, n * 128 : n * 128 + 128]
            pair = swap(cols[:count], cols[count:])
            ob[2 * n, at : at + count], ob[2 * n + 1, at : at + count] = [v.astype(BF16) for v in pair]
            send_back(part, (2 * n, 2 * n + 1))

    def send_back(part, quarters):
        for j in PARTS[part]:
            z_to = j * Q + z_low
            for cs in range(2):
                for qs in quarters:
                    copy = pltpu.make_async_remote_copy(
                        src_ref=ob.at[qs, tile(rows_at(j, cs))],
                        dst_ref=rb.at[tile(ep * 16)],
                        send_sem=ret_send.at[(j * 2 + cs) * Q + qs],
                        recv_sem=ret_recv.at[ep],
                        device_id=(z_to * 2 + cs, place(c, qs, column)),
                        device_id_type=MESH,
                    )
                    if qs == 0:
                        own = is_own(j, cs)

                        @pl.when(jnp.logical_not(own))
                        def _():
                            copy.start()

                        @pl.when(own)
                        def _():
                            rb[tile(ep * 16), :] = ob[0, tile(rows_at(j, cs)), :]
                        sends.append((copy, own))
                    else:
                        copy.start()
                        sends.append((copy, None))

    pass_rows(0)
    pass_rows(1)
    pass_rows(2)
    x_parts[0].finish()
    gu.finish()
    make_hidden(0)
    x_parts[1].finish()
    make_hidden(1)
    dn.finish()
    for k in range(2):
        @pl.when(c == k)
        def _():
            order_down(k)
    x_parts[2].finish()
    make_hidden(2)
    make_result(0)
    make_result(1)
    make_result(2)

    for dz in range(NZ):
        for ce in range(2):
            e = ((z + dz) % NZ) * 2 + ce
            arrived = pltpu.make_async_remote_copy(
                src_ref=ob.at[0, tile(0)],
                dst_ref=rb.at[tile(e * 16)],
                send_sem=ret_send.at[0],
                recv_sem=ret_recv.at[e],
                device_id=(ep, tp),
                device_id_type=MESH,
            )
            if dz == 0:
                @pl.when(jnp.logical_not(jnp.logical_and(quarter_of[ce] == 0, c == ce)))
                def _():
                    arrived.wait_recv()
            else:
                arrived.wait_recv()

    mixed = dot_columns(rb[...], mixer[...])
    combined = mixed[0:HALF, 0:128] + mixed[HALF:128, 384:512]
    for i in range(1, 3):
        combined = combined + mixed[0:HALF, i * 128 : i * 128 + 128]
        combined = combined + mixed[HALF:128, 384 + i * 128 : 512 + i * 128]
    out_ref[...] = combined.astype(BF16)

    for copy, own in sends:
        if own is None:
            copy.wait_send()
        else:
            @pl.when(jnp.logical_not(own))
            def _():
                copy.wait_send()
    for gather in [gu, dn] + x_parts + h_parts:
        gather.drain()


def body(tokens, norm_gain, gate_weight, up_weight, down_weight, expert_ids, route_weight):
    turned = (0, 2, 1)
    return pl.pallas_call(
        kernel,
        out_shape=jax.ShapeDtypeStruct((HALF, TOK), BF16),
        in_specs=[pl.BlockSpec(memory_space=pl.ANY)] * 7,
        out_specs=pl.BlockSpec(memory_space=pltpu.VMEM),
        scratch_shapes=[
            pltpu.VMEM((HALF, TOK), BF16),
            pltpu.VMEM((8, 128), F32),
            pltpu.VMEM((TOPK, TOK), jnp.int32),
            pltpu.VMEM((TOPK, TOK), F32),
            pltpu.VMEM((512, 128), BF16),
            pltpu.VMEM((Q, 128, D), BF16),
            pltpu.VMEM((Q, HALF, D), BF16),
            pltpu.VMEM((Q, 256, 256), BF16),
            pltpu.VMEM((Q, Q, 128, 128), BF16),
            pltpu.VMEM((Q, 2, 256, 128), BF16),
            pltpu.VMEM((Q, 128, 128), BF16),
            pltpu.VMEM((512, 128), BF16),
            pltpu.VMEM((512, 768), BF16),
            pltpu.SemaphoreType.DMA((7,)),
            pltpu.SemaphoreType.DMA((32,)),
            pltpu.SemaphoreType.DMA((32,)),
            pltpu.SemaphoreType.DMA((32,)),
            pltpu.SemaphoreType.DMA((32,)),
            pltpu.SemaphoreType.DMA((12 + 12 * N_PART,)),
            pltpu.SemaphoreType.DMA((12 + 12 * N_PART,)),
        ],
        compiler_params=pltpu.CompilerParams(collective_id=0, has_side_effects=True),
    )(
        tokens.T, norm_gain.reshape(8, 128), gate_weight.transpose(turned), up_weight.transpose(turned),
        down_weight.transpose(turned), expert_ids.T, route_weight.T,
    ).T


def solution(mesh):
    in_specs = (
        P("ep", "tp"),
        P(),
        P("ep", None, "tp"),
        P("ep", None, "tp"),
        P("ep", None, "tp"),
        P("ep", None),
        P("ep", None),
    )
    return jax.shard_map(body, mesh=mesh, in_specs=in_specs, out_specs=P("ep", "tp"), check_vma=False)
```

```python
import jax
import jax.numpy as jnp
from jax import lax
from jax.experimental import pallas as pl
from jax.experimental.pallas import tpu as pltpu
from jax.sharding import PartitionSpec as P

MESH = pl.DeviceIdType.MESH
F32 = jnp.float32
BF16 = jnp.bfloat16

EPSILON = 1e-06
ALPHA = 1.702
LIMIT = 7.0

NZ = 16
Q = 4
D = 1024
TOK = 128
EXPERTS = 32
TOPK = 4
HALF = 64
Z_ORDER = (8, 7, 9, 6, 10, 5, 11, 4, 12, 3, 13, 2, 14, 1, 15, 0)
PARTS = ((0,), (1,), (2, 3))
N_PART = len(PARTS)


def iota(shape, dim):
    return lax.broadcasted_iota(jnp.int32, shape, dim)


def dot(a, b):
    return jnp.dot(a, b, preferred_element_type=F32)


def dot_rows(a, b):
    return lax.dot_general(a, b, (((1,), (1,)), ((), ())), preferred_element_type=F32)


def dot_columns(a, b):
    return lax.dot_general(a, b, (((0,), (0,)), ((), ())), preferred_element_type=F32)


def placed(offset):
    return jnp.where(iota((HALF, 128), 1) == iota((HALF, 128), 0) + offset, 1.0, 0.0).astype(BF16)


def swap(a, b):
    low = iota(a.shape, 1) < HALF
    return jnp.where(low, a, pltpu.roll(b, HALF, 1)), jnp.where(low, pltpu.roll(a, HALF, 1), b)


def bits(v):
    return v // 2, ((v + 1) % Q) // 2


def gray(a, b):
    return 3 * a + b - 2 * a * b


def place(k, quarter, column):
    if isinstance(k, int):
        a, b = (column, quarter) if k == 0 else (quarter, column)
    else:
        a = column + k * (quarter - column)
        b = quarter + k * (column - quarter)
    return gray(a // 2, b // 2) * Q + gray(a % 2, b % 2)


def rows_at(j, core):
    return (j * 2 + core) * 16


def tile(start):
    return pl.ds(start if isinstance(start, int) else pl.multiple_of(start, 16), 16)


def sized(ref, sem, device):
    return pltpu.make_async_remote_copy(
        src_ref=ref, dst_ref=ref, send_sem=sem, recv_sem=sem, device_id=device, device_id_type=MESH
    )


class Square:
    def __init__(self, view, mine, device, send_sem, recv_sems):
        self.view, self.device = view, device
        self.send_sem, self.recv_sems = send_sem, recv_sems
        self.mine = mine
        self.right = mine + 1 - 2 * (mine % 2)
        self.left = mine + 2 - 4 * (mine // 2)
        self.far = 3 - mine
        self.others = (self.far, self.right, self.left)

    def send(self, owner, h, to, index):
        pltpu.make_async_remote_copy(
            src_ref=self.view(owner, h),
            dst_ref=self.view(owner, h),
            send_sem=self.send_sem,
            recv_sem=self.recv_sems.at[index],
            device_id=self.device(to),
            device_id_type=MESH,
        ).start()

    def arrived(self, ref, index):
        sized(ref, self.recv_sems.at[index], self.device(self.right)).wait_recv()


class Gather(Square):
    def start(self):
        self.send(self.mine, 0, self.right, 0)
        self.send(self.mine, 1, self.left, 1)
        self.send(self.mine, 1, self.right, 2)
        self.send(self.mine, 0, self.left, 2)

    def forward(self):
        self.arrived(self.view(self.right, 0), 0)
        self.send(self.right, 0, self.left, 2)
        self.arrived(self.view(self.left, 1), 1)
        self.send(self.left, 1, self.right, 2)


class Exchange(Square):
    def __init__(self, *args, apart):
        super().__init__(*args)
        self.apart = apart

    def send_all(self, h):
        for index, to in enumerate(self.others):
            self.send(self.mine, h, to, index if self.apart else 0)


def kernel(
    tok_hbm, gain_hbm, gate_hbm, up_hbm, down_hbm, ids_hbm, rw_hbm, out_ref,
    tok, gain, ids, rw,
    pbuf, gub, dnb, dnf, xb, hb, ob, rb, mixer,
    in_sem, disp_send, disp_recv, ret_send, ret_recv, send_sems, gu_recv, dn_recv, x_recv, h_recv,
):
    ep = lax.axis_index("ep")
    tp = lax.axis_index("tp")
    z, c = ep // 2, ep % 2
    (ay, by), (ax, bx) = bits(tp // Q), bits(tp % Q)
    side_a, side_b = ay * 2 + ax, by * 2 + bx
    quarter_of, column_of = (side_b, side_a), (side_a, side_b)
    quarter = side_b + c * (side_a - side_b)
    column = side_a + c * (side_b - side_a)

    barrier = pltpu.get_barrier_semaphore()

    def greet(device):
        pl.semaphore_signal(barrier, inc=1, device_id=device, device_id_type=MESH)

    def with_column(to):
        return (ep, place(c, to, column))

    def with_quarter(to):
        return (ep, place(c, quarter, to))

    z_low = (z - quarter + NZ) % Q

    def is_own(j, cs):
        return jnp.logical_and(jnp.logical_and(quarter == 0, c == cs), z // Q == j)

    for j in range(Q):
        z_from = j * Q + z_low
        for cs in range(2):
            for qs in range(Q):
                device = (z_from * 2 + cs, place(c, qs, column))
                if qs == 0:
                    @pl.when(jnp.logical_not(is_own(j, cs)))
                    def _():
                        greet(device)
                else:
                    greet(device)

    loads = []
    for i, (src, dst) in enumerate(
        ((ids_hbm, ids), (tok_hbm, tok), (gate_hbm.at[0], gub.at[quarter, pl.ds(0, HALF)]),
         (up_hbm.at[0], gub.at[quarter, pl.ds(HALF, HALF)]), (down_hbm.at[0], dnb.at[quarter]),
         (gain_hbm, gain), (rw_hbm, rw))
    ):
        load = pltpu.make_async_copy(src, dst, in_sem.at[i])
        load.start()
        loads.append(load)

    gu = Gather(
        lambda o, h: gub.at[o, pl.ds(h * HALF, HALF)], quarter, with_column, send_sems.at[0], gu_recv
    )
    dn = Gather(
        lambda o, h: dnb.at[o, pl.ds(h * 32, 32)], quarter, with_column, send_sems.at[1], dn_recv
    )
    x_parts, h_parts = [], []
    for i, part in enumerate(PARTS):
        x_parts.append(Exchange(
            lambda o, h, first=part[0]: xb.at[o, :, pl.ds((first + h) * 32, 32)],
            column, with_quarter, send_sems.at[2], x_recv.at[pl.ds(i, 1)], apart=False,
        ))
        h_parts.append(Exchange(
            lambda o, h, part=part: hb.at[o, h, pl.ds(part[0] * 64, len(part) * 64)],
            column, with_quarter, send_sems.at[3], h_recv.at[i], apart=True,
        ))
    for gather in (gu, x_parts[0]):
        greet(gather.device(gather.right))
        greet(gather.device(gather.left))
    greet(x_parts[0].device(x_parts[0].far))

    loads[0].wait()
    experts = iota((EXPERTS, TOK), 0)
    named = [ids[k : k + 1, :] == experts for k in range(TOPK)]
    member = named[0] | named[1] | named[2] | named[3]
    earlier = jnp.where(iota((TOK, TOK), 0) < iota((TOK, TOK), 1), 1.0, 0.0).astype(BF16)
    slot = dot(jnp.where(member, 1.0, 0.0).astype(BF16), earlier)
    code = jnp.where(member, slot, -1.0).astype(BF16)
    expand = jnp.where(iota((512, EXPERTS), 0) // 16 == iota((512, EXPERTS), 1), 1.0, 0.0).astype(BF16)
    code_wide = dot(expand, code)
    slot_of_row = (iota((512, TOK), 0) % 16).astype(F32)
    pick_low = jnp.where(code_wide == slot_of_row, 1.0, 0.0)
    pick_high = jnp.where(code_wide == slot_of_row + 16.0, 1.0, 0.0)

    loads[1].wait()
    token_low = dot_columns(tok[...], placed(0)).astype(BF16)
    token_high = dot_columns(tok[...], placed(HALF)).astype(BF16)
    packed = dot(pick_low.astype(BF16), token_low) + dot(pick_high.astype(BF16), token_high)
    pbuf[...] = packed.astype(BF16)

    pl.semaphore_wait(barrier, 2 * NZ + 5 - jnp.where(quarter == 0, 1, 0))

    def is_mine(dz, ce):
        return jnp.logical_and(quarter == 0, c == ce) if dz == 0 else None

    def dispatch():
        for dz in Z_ORDER:
            for ce in range(2):
                e = ((z + dz) % NZ) * 2 + ce
                copy = pltpu.make_async_remote_copy(
                    src_ref=pbuf.at[tile(e * 16)],
                    dst_ref=xb.at[column_of[ce], quarter_of[ce], tile(rows_at(z // Q, c))],
                    send_sem=disp_send,
                    recv_sem=disp_recv.at[z // Q],
                    device_id=(e, place(ce, dz % Q, column_of[ce])),
                    device_id_type=MESH,
                )
                if dz == 0:
                    @pl.when(jnp.logical_not(is_mine(dz, ce)))
                    def _():
                        copy.start()

                    @pl.when(is_mine(dz, ce))
                    def _():
                        xb[column, 0, tile(rows_at(z // Q, c)), :] = pbuf[tile(e * 16), :]
                else:
                    copy.start()

    dispatch()

    for load in loads[2:5]:
        load.wait()
    gu.start()
    dn.start()

    loads[5].wait()
    loads[6].wait()
    weight = jnp.zeros((EXPERTS, TOK), F32)
    for k in range(TOPK):
        weight = weight + jnp.where(named[k], rw[k : k + 1, :], 0.0)
    for i in range(3):
        piece = weight.astype(BF16)
        weight = weight - piece.astype(F32)
        wide = dot(expand, piece)
        mixer[:, i * 128 : i * 128 + 128] = (wide * pick_low).astype(BF16)
        mixer[:, 384 + i * 128 : 512 + i * 128] = (wide * pick_high).astype(BF16)

    gu.forward()
    dn.forward()

    def all_but_own(own, whole, rest, sem, wait):
        @pl.when(jnp.logical_not(own))
        def _():
            wait(sized(whole, sem, (ep, tp)))

        @pl.when(own)
        def _():
            wait(sized(rest, sem, (ep, tp)))

    def pass_rows(part):
        for h, j in enumerate(PARTS[part]):
            all_but_own(
                jnp.logical_and(quarter == 0, z // Q == j),
                xb.at[column, :, pl.ds(j * 32, 32)], pbuf.at[pl.ds(0, 112)],
                disp_recv.at[j], lambda copy: copy.wait_recv(),
            )
            x_parts[part].send_all(h)

    def x_arrived(part):
        js = PARTS[part]
        x_parts[part].arrived(xb.at[pl.ds(0, 3), :, pl.ds(js[0] * 32, len(js) * 32)], 0)

    def slice_at(s, part):
        (ty, uy), (tx, ux) = bits(s // Q), bits(s % Q)
        t, u = ty * 2 + tx, uy * 2 + ux
        first, last = PARTS[part][0] * 32, PARTS[part][-1] * 32 + 32
        return xb[t + c * (u - t), u + c * (t - u), first:last].astype(F32)

    def make_hidden(part):
        groups = []
        at, count = PARTS[part][0] * 64, len(PARTS[part]) * 64
        square = jnp.zeros((count, 128), F32)
        for g in range(8):
            low, high = swap(slice_at(2 * g, part), slice_at(2 * g + 1, part))
            both = jnp.concatenate([low, high], axis=0)
            square = square + both * both
            groups.append(both)
        inverse = lax.rsqrt(jnp.sum(square, axis=1, keepdims=True) / D + EPSILON)
        rows = jnp.concatenate(
            [(groups[g] * inverse * gain[g : g + 1, :]).astype(BF16) for g in range(8)], axis=1
        )
        for p in range(2):
            both = dot_rows(rows, jnp.concatenate([gub[2 * p], gub[2 * p + 1]], axis=0))
            gate_pre, up_pre = swap(both[:, :128], both[:, 128:])
            gate_pre = jnp.minimum(gate_pre, LIMIT)
            up_pre = jnp.clip(up_pre, -LIMIT, LIMIT)
            hidden = (up_pre + 1.0) * gate_pre * jax.nn.sigmoid(ALPHA * gate_pre)
            hb[column, p, at : at + count] = hidden.astype(BF16)
            h_parts[part].send_all(p)

    def order_down(k):
        low = iota((HALF, 128), 1) < HALF
        for n in range(Q):
            for o in range(Q):
                for p in range(2):
                    sides = []
                    for h in range(2):
                        s = place(k, 2 * p + h, o)
                        v = dnb[n, :, s // 2 * 128 : s // 2 * 128 + 128].astype(F32)
                        sides.append(v if s % 2 == h else pltpu.roll(v, HALF, 1))
                    dnf[o, n * HALF : n * HALF + HALF, p * 128 : p * 128 + 128] = jnp.where(low, *sides).astype(BF16)

    def make_result(part):
        exchange = h_parts[part]
        at, count = PARTS[part][0] * 32, len(PARTS[part]) * 32

        def term(owner):
            units = jnp.concatenate([hb[owner, p, 2 * at : 2 * at + 2 * count] for p in range(2)], axis=1)
            return dot_rows(units, dnf[owner])

        result = term(column)
        for index in (1, 2, 0):
            owner = exchange.others[index]
            exchange.arrived(hb.at[owner, :, pl.ds(2 * at, 2 * count)], index)
            result = result + term(owner)
        for n in range(2):
            cols = result[:, n * 128 : n * 128 + 128]
            pair = swap(cols[:count], cols[count:])
            ob[2 * n, at : at + count], ob[2 * n + 1, at : at + count] = [v.astype(BF16) for v in pair]
            send_back(part, (2 * n, 2 * n + 1))

    def send_back(part, quarters):
        for j in PARTS[part]:
            z_to = j * Q + z_low
            for cs in range(2):
                for qs in quarters:
                    copy = pltpu.make_async_remote_copy(
                        src_ref=ob.at[qs, tile(rows_at(j, cs))],
                        dst_ref=rb.at[tile(ep * 16)],
                        send_sem=ret_send,
                        recv_sem=ret_recv,
                        device_id=(z_to * 2 + cs, place(c, qs, column)),
                        device_id_type=MESH,
                    )
                    if qs == 0:
                        own = is_own(j, cs)

                        @pl.when(jnp.logical_not(own))
                        def _():
                            copy.start()

                        @pl.when(own)
                        def _():
                            rb[tile(ep * 16), :] = ob[0, tile(rows_at(j, cs)), :]
                    else:
                        copy.start()

    pass_rows(0)
    pass_rows(1)
    pass_rows(2)
    x_arrived(0)
    gu.arrived(gub.at[pl.ds(0, 2)], 2)
    make_hidden(0)
    x_arrived(1)
    make_hidden(1)
    dn.arrived(dnb.at[pl.ds(0, 2)], 2)
    for k in range(2):
        @pl.when(c == k)
        def _():
            order_down(k)
    x_arrived(2)
    make_hidden(2)
    make_result(0)
    make_result(1)
    make_result(2)

    all_but_own(
        quarter == 0, rb, rb.at[pl.ds(0, 496)], ret_recv, lambda copy: copy.wait_recv()
    )

    mixed = dot_columns(rb[...], mixer[...])
    combined = mixed[0:HALF, 0:128] + mixed[HALF:128, 384:512]
    for i in range(1, 3):
        combined = combined + mixed[0:HALF, i * 128 : i * 128 + 128]
        combined = combined + mixed[HALF:128, 384 + i * 128 : 512 + i * 128]
    out_ref[...] = combined.astype(BF16)

    for sem in (disp_send, ret_send):
        all_but_own(quarter == 0, rb, rb.at[pl.ds(0, 496)], sem, lambda copy: copy.wait_send())
    for i, buf in enumerate((gub, dnb, xb, hb)):
        sized(buf.at[pl.ds(0, 3)], send_sems.at[i], (ep, tp)).wait_send()


def body(tokens, norm_gain, gate_weight, up_weight, down_weight, expert_ids, route_weight):
    turned = (0, 2, 1)
    return pl.pallas_call(
        kernel,
        out_shape=pltpu.VMEM((HALF, TOK), BF16),
        in_specs=[pl.BlockSpec(memory_space=pl.ANY)] * 7,
        out_specs=pl.BlockSpec(memory_space=pltpu.VMEM),
        scratch_shapes=[
            pltpu.VMEM((HALF, TOK), BF16),
            pltpu.VMEM((8, 128), F32),
            pltpu.VMEM((TOPK, TOK), jnp.int32),
            pltpu.VMEM((TOPK, TOK), F32),
            pltpu.VMEM((512, 128), BF16),
            pltpu.VMEM((Q, 128, D), BF16),
            pltpu.VMEM((Q, HALF, D), BF16),
            pltpu.VMEM((Q, 256, 256), BF16),
            pltpu.VMEM((Q, Q, 128, 128), BF16),
            pltpu.VMEM((Q, 2, 256, 128), BF16),
            pltpu.VMEM((Q, 128, 128), BF16),
            pltpu.VMEM((512, 128), BF16),
            pltpu.VMEM((512, 768), BF16),
            pltpu.SemaphoreType.DMA((7,)),
            pltpu.SemaphoreType.DMA,
            pltpu.SemaphoreType.DMA((Q,)),
            pltpu.SemaphoreType.DMA,
            pltpu.SemaphoreType.DMA,
            pltpu.SemaphoreType.DMA((4,)),
            pltpu.SemaphoreType.DMA((3,)),
            pltpu.SemaphoreType.DMA((3,)),
            pltpu.SemaphoreType.DMA((N_PART,)),
            pltpu.SemaphoreType.DMA((N_PART, 3)),
        ],
        compiler_params=pltpu.CompilerParams(collective_id=0, has_side_effects=True),
    )(
        tokens.T, norm_gain.reshape(8, 128), gate_weight.transpose(turned), up_weight.transpose(turned),
        down_weight.transpose(turned), expert_ids.T, route_weight.T,
    ).T


def solution(mesh):
    in_specs = (
        P("ep", "tp"),
        P(),
        P("ep", None, "tp"),
        P("ep", None, "tp"),
        P("ep", None, "tp"),
        P("ep", None),
        P("ep", None),
    )
    return jax.shard_map(body, mesh=mesh, in_specs=in_specs, out_specs=P("ep", "tp"), check_vma=False)
```

```python
import jax
import jax.numpy as jnp
from jax import lax
from jax.experimental import pallas as pl
from jax.experimental.pallas import tpu as pltpu
from jax.sharding import PartitionSpec as P

MESH = pl.DeviceIdType.MESH
F32 = jnp.float32
BF16 = jnp.bfloat16

EPSILON = 1e-06
ALPHA = 1.702
LIMIT = 7.0

NZ = 16
Q = 4
D = 1024
TOK = 128
EXPERTS = 32
TOPK = 4
HALF = 64
LATE_FROM = 8
Z_ORDER = (8, 7, 9, 6, 10, 5, 11, 4, 12, 3, 13, 2, 14, 1, 15, 0)
PARTS = ((0,), (1,), (2, 3))
N_PART = len(PARTS)


def iota(shape, dim):
    return lax.broadcasted_iota(jnp.int32, shape, dim)


def dot(a, b):
    return jnp.dot(a, b, preferred_element_type=F32)


def dot_rows(a, b):
    return lax.dot_general(a, b, (((1,), (1,)), ((), ())), preferred_element_type=F32)


def dot_columns(a, b):
    return lax.dot_general(a, b, (((0,), (0,)), ((), ())), preferred_element_type=F32)


def placed(offset):
    return jnp.where(iota((HALF, 128), 1) == iota((HALF, 128), 0) + offset, 1.0, 0.0).astype(BF16)


def swap(a, b):
    low = iota(a.shape, 1) < HALF
    return jnp.where(low, a, pltpu.roll(b, HALF, 1)), jnp.where(low, pltpu.roll(a, HALF, 1), b)


def bits(v):
    return v // 2, ((v + 1) % Q) // 2


def gray(a, b):
    return 3 * a + b - 2 * a * b


def place(k, quarter, column):
    if isinstance(k, int):
        a, b = (column, quarter) if k == 0 else (quarter, column)
    else:
        a = column + k * (quarter - column)
        b = quarter + k * (column - quarter)
    return gray(a // 2, b // 2) * Q + gray(a % 2, b % 2)


def rows_at(j, core):
    return (j * 2 + core) * 16


def tile(start):
    return pl.ds(start if isinstance(start, int) else pl.multiple_of(start, 16), 16)


def sized(ref, sem, device):
    return pltpu.make_async_remote_copy(
        src_ref=ref, dst_ref=ref, send_sem=sem, recv_sem=sem, device_id=device, device_id_type=MESH
    )


class Square:
    def __init__(self, view, mine, device, send_sem, recv_sems):
        self.view, self.device = view, device
        self.send_sem, self.recv_sems = send_sem, recv_sems
        self.mine = mine
        self.right = mine + 1 - 2 * (mine % 2)
        self.left = mine + 2 - 4 * (mine // 2)
        self.far = 3 - mine
        self.others = (self.far, self.right, self.left)

    def send(self, owner, h, to, index):
        pltpu.make_async_remote_copy(
            src_ref=self.view(owner, h),
            dst_ref=self.view(owner, h),
            send_sem=self.send_sem,
            recv_sem=self.recv_sems.at[index],
            device_id=self.device(to),
            device_id_type=MESH,
        ).start()

    def arrived(self, ref, index):
        sized(ref, self.recv_sems.at[index], self.device(self.right)).wait_recv()


class Gather(Square):
    def start(self):
        self.send(self.mine, 0, self.right, 0)
        self.send(self.mine, 1, self.left, 1)
        self.send(self.mine, 1, self.right, 2)
        self.send(self.mine, 0, self.left, 2)

    def forward(self):
        self.arrived(self.view(self.right, 0), 0)
        self.send(self.right, 0, self.left, 2)
        self.arrived(self.view(self.left, 1), 1)
        self.send(self.left, 1, self.right, 2)


class Exchange(Square):
    def __init__(self, *args, apart):
        super().__init__(*args)
        self.apart = apart

    def send_all(self, h):
        for index, to in enumerate(self.others):
            self.send(self.mine, h, to, index if self.apart else 0)


def kernel(
    tok_hbm, gain_hbm, gate_hbm, up_hbm, down_hbm, ids_hbm, rw_hbm, out_ref,
    tok, gain, ids, rw,
    pbuf, gub, dnb, dnf, xb, hb, ob, rb, mixer,
    in_sem, disp_send, disp_recv, ret_send, ret_recv, send_sems, gu_recv, dn_recv, x_recv, h_recv,
):
    ep = lax.axis_index("ep")
    tp = lax.axis_index("tp")
    z, c = ep // 2, ep % 2
    (ay, by), (ax, bx) = bits(tp // Q), bits(tp % Q)
    side_a, side_b = ay * 2 + ax, by * 2 + bx
    quarter_of, column_of = (side_b, side_a), (side_a, side_b)
    quarter = side_b + c * (side_a - side_b)
    column = side_a + c * (side_b - side_a)

    barrier = pltpu.get_barrier_semaphore()

    def greet(device):
        pl.semaphore_signal(barrier, inc=1, device_id=device, device_id_type=MESH)

    def with_column(to):
        return (ep, place(c, to, column))

    def with_quarter(to):
        return (ep, place(c, quarter, to))

    z_low = (z - quarter + NZ) % Q

    def is_own(j, cs):
        return jnp.logical_and(jnp.logical_and(quarter == 0, c == cs), z // Q == j)

    for j in range(Q):
        z_from = j * Q + z_low
        for cs in range(2):
            for qs in range(Q):
                device = (z_from * 2 + cs, place(c, qs, column))
                if qs == 0:
                    @pl.when(jnp.logical_not(is_own(j, cs)))
                    def _():
                        greet(device)
                else:
                    greet(device)

    loads = []
    for i, (src, dst) in enumerate(
        ((ids_hbm, ids), (tok_hbm, tok), (gate_hbm.at[0], gub.at[quarter, pl.ds(0, HALF)]),
         (up_hbm.at[0], gub.at[quarter, pl.ds(HALF, HALF)]), (down_hbm.at[0], dnb.at[quarter]),
         (gain_hbm, gain), (rw_hbm, rw))
    ):
        load = pltpu.make_async_copy(src, dst, in_sem.at[i])
        load.start()
        loads.append(load)

    gu = Gather(
        lambda o, h: gub.at[o, pl.ds(h * HALF, HALF)], quarter, with_column, send_sems.at[0], gu_recv
    )
    dn = Gather(
        lambda o, h: dnb.at[o, pl.ds(h * 32, 32)], quarter, with_column, send_sems.at[1], dn_recv
    )
    x_parts, h_parts = [], []
    for i, part in enumerate(PARTS):
        x_parts.append(Exchange(
            lambda o, h, first=part[0]: xb.at[o, :, pl.ds((first + h) * 32, 32)],
            column, with_quarter, send_sems.at[2], x_recv.at[pl.ds(i, 1)], apart=False,
        ))
        h_parts.append(Exchange(
            lambda o, h, part=part: hb.at[o, h, pl.ds(part[0] * 64, len(part) * 64)],
            column, with_quarter, send_sems.at[3], h_recv.at[i], apart=True,
        ))
    for gather in (gu, x_parts[0]):
        greet(gather.device(gather.right))
        greet(gather.device(gather.left))
    greet(x_parts[0].device(x_parts[0].far))

    loads[0].wait()
    experts = iota((EXPERTS, TOK), 0)
    named = [ids[k : k + 1, :] == experts for k in range(TOPK)]
    member = named[0] | named[1] | named[2] | named[3]
    earlier = jnp.where(iota((TOK, TOK), 0) < iota((TOK, TOK), 1), 1.0, 0.0).astype(BF16)
    slot = dot(jnp.where(member, 1.0, 0.0).astype(BF16), earlier)
    code = jnp.where(member, slot, -1.0).astype(BF16)
    expand = jnp.where(iota((512, EXPERTS), 0) // 16 == iota((512, EXPERTS), 1), 1.0, 0.0).astype(BF16)
    code_wide = dot(expand, code)
    slot_of_row = (iota((512, TOK), 0) % 16).astype(F32)
    pick_low = jnp.where(code_wide == slot_of_row, 1.0, 0.0)
    pick_high = jnp.where(code_wide == slot_of_row + 16.0, 1.0, 0.0)

    loads[1].wait()
    token_low = dot_columns(tok[...], placed(0)).astype(BF16)
    token_high = dot_columns(tok[...], placed(HALF)).astype(BF16)
    packed = dot(pick_low.astype(BF16), token_low) + dot(pick_high.astype(BF16), token_high)
    pbuf[...] = packed.astype(BF16)

    pl.semaphore_wait(barrier, 2 * NZ + 5 - jnp.where(quarter == 0, 1, 0))

    def is_mine(dz, ce):
        return jnp.logical_and(quarter == 0, c == ce) if dz == 0 else None

    def dispatch():
        for dz in Z_ORDER:
            for ce in range(2):
                e = ((z + dz) % NZ) * 2 + ce
                copy = pltpu.make_async_remote_copy(
                    src_ref=pbuf.at[tile(e * 16)],
                    dst_ref=xb.at[column_of[ce], quarter_of[ce], tile(rows_at(z // Q, c))],
                    send_sem=disp_send,
                    recv_sem=disp_recv.at[z // Q],
                    device_id=(e, place(ce, dz % Q, column_of[ce])),
                    device_id_type=MESH,
                )
                if dz == 0:
                    @pl.when(jnp.logical_not(is_mine(dz, ce)))
                    def _():
                        copy.start()

                    @pl.when(is_mine(dz, ce))
                    def _():
                        xb[column, 0, tile(rows_at(z // Q, c)), :] = pbuf[tile(e * 16), :]
                else:
                    copy.start()

    pl.when(z < LATE_FROM)(dispatch)

    for load in loads[2:5]:
        load.wait()
    gu.start()
    dn.start()

    loads[5].wait()
    loads[6].wait()
    weight = jnp.zeros((EXPERTS, TOK), F32)
    for k in range(TOPK):
        weight = weight + jnp.where(named[k], rw[k : k + 1, :], 0.0)
    for i in range(3):
        piece = weight.astype(BF16)
        weight = weight - piece.astype(F32)
        wide = dot(expand, piece)
        mixer[:, i * 128 : i * 128 + 128] = (wide * pick_low).astype(BF16)
        mixer[:, 384 + i * 128 : 512 + i * 128] = (wide * pick_high).astype(BF16)

    pl.when(z >= LATE_FROM)(dispatch)
    gu.forward()
    dn.forward()

    def all_but_own(own, whole, rest, sem, wait):
        @pl.when(jnp.logical_not(own))
        def _():
            wait(sized(whole, sem, (ep, tp)))

        @pl.when(own)
        def _():
            wait(sized(rest, sem, (ep, tp)))

    def pass_rows(part):
        for h, j in enumerate(PARTS[part]):
            all_but_own(
                jnp.logical_and(quarter == 0, z // Q == j),
                xb.at[column, :, pl.ds(j * 32, 32)], pbuf.at[pl.ds(0, 112)],
                disp_recv.at[j], lambda copy: copy.wait_recv(),
            )
            x_parts[part].send_all(h)

    def x_arrived(part):
        js = PARTS[part]
        x_parts[part].arrived(xb.at[pl.ds(0, 3), :, pl.ds(js[0] * 32, len(js) * 32)], 0)

    def slice_at(s, part):
        (ty, uy), (tx, ux) = bits(s // Q), bits(s % Q)
        t, u = ty * 2 + tx, uy * 2 + ux
        first, last = PARTS[part][0] * 32, PARTS[part][-1] * 32 + 32
        return xb[t + c * (u - t), u + c * (t - u), first:last].astype(F32)

    def make_hidden(part):
        groups = []
        at, count = PARTS[part][0] * 64, len(PARTS[part]) * 64
        square = jnp.zeros((count, 128), F32)
        for g in range(8):
            low, high = swap(slice_at(2 * g, part), slice_at(2 * g + 1, part))
            both = jnp.concatenate([low, high], axis=0)
            square = square + both * both
            groups.append(both)
        inverse = lax.rsqrt(jnp.sum(square, axis=1, keepdims=True) / D + EPSILON)
        rows = jnp.concatenate(
            [(groups[g] * inverse * gain[g : g + 1, :]).astype(BF16) for g in range(8)], axis=1
        )
        for p in range(2):
            both = dot_rows(rows, jnp.concatenate([gub[2 * p], gub[2 * p + 1]], axis=0))
            gate_pre, up_pre = swap(both[:, :128], both[:, 128:])
            gate_pre = jnp.minimum(gate_pre, LIMIT)
            up_pre = jnp.clip(up_pre, -LIMIT, LIMIT)
            hidden = (up_pre + 1.0) * gate_pre * jax.nn.sigmoid(ALPHA * gate_pre)
            hb[column, p, at : at + count] = hidden.astype(BF16)
            h_parts[part].send_all(p)

    def order_down(k):
        low = iota((HALF, 128), 1) < HALF
        for n in range(Q):
            for o in range(Q):
                for p in range(2):
                    sides = []
                    for h in range(2):
                        s = place(k, 2 * p + h, o)
                        v = dnb[n, :, s // 2 * 128 : s // 2 * 128 + 128].astype(F32)
                        sides.append(v if s % 2 == h else pltpu.roll(v, HALF, 1))
                    dnf[o, n * HALF : n * HALF + HALF, p * 128 : p * 128 + 128] = jnp.where(low, *sides).astype(BF16)

    def make_result(part):
        exchange = h_parts[part]
        at, count = PARTS[part][0] * 32, len(PARTS[part]) * 32

        def term(owner):
            units = jnp.concatenate([hb[owner, p, 2 * at : 2 * at + 2 * count] for p in range(2)], axis=1)
            return dot_rows(units, dnf[owner])

        result = term(column)
        for index in (1, 2, 0):
            owner = exchange.others[index]
            exchange.arrived(hb.at[owner, :, pl.ds(2 * at, 2 * count)], index)
            result = result + term(owner)
        for n in range(2):
            cols = result[:, n * 128 : n * 128 + 128]
            pair = swap(cols[:count], cols[count:])
            ob[2 * n, at : at + count], ob[2 * n + 1, at : at + count] = [v.astype(BF16) for v in pair]
            send_back(part, (2 * n, 2 * n + 1))

    def send_back(part, quarters):
        for j in PARTS[part]:
            z_to = j * Q + z_low
            for cs in range(2):
                for qs in quarters:
                    copy = pltpu.make_async_remote_copy(
                        src_ref=ob.at[qs, tile(rows_at(j, cs))],
                        dst_ref=rb.at[tile(ep * 16)],
                        send_sem=ret_send,
                        recv_sem=ret_recv,
                        device_id=(z_to * 2 + cs, place(c, qs, column)),
                        device_id_type=MESH,
                    )
                    if qs == 0:
                        own = is_own(j, cs)

                        @pl.when(jnp.logical_not(own))
                        def _():
                            copy.start()

                        @pl.when(own)
                        def _():
                            rb[tile(ep * 16), :] = ob[0, tile(rows_at(j, cs)), :]
                    else:
                        copy.start()

    pass_rows(0)
    pass_rows(1)
    pass_rows(2)
    x_arrived(0)
    gu.arrived(gub.at[pl.ds(0, 2)], 2)
    make_hidden(0)
    x_arrived(1)
    make_hidden(1)
    dn.arrived(dnb.at[pl.ds(0, 2)], 2)
    for k in range(2):
        @pl.when(c == k)
        def _():
            order_down(k)
    make_result(0)
    x_arrived(2)
    make_hidden(2)
    make_result(1)
    make_result(2)

    all_but_own(
        quarter == 0, rb, rb.at[pl.ds(0, 496)], ret_recv, lambda copy: copy.wait_recv()
    )

    mixed = dot_columns(rb[...], mixer[...])
    combined = mixed[0:HALF, 0:128] + mixed[HALF:128, 384:512]
    for i in range(1, 3):
        combined = combined + mixed[0:HALF, i * 128 : i * 128 + 128]
        combined = combined + mixed[HALF:128, 384 + i * 128 : 512 + i * 128]
    out_ref[...] = combined.astype(BF16)

    for sem in (disp_send, ret_send):
        all_but_own(quarter == 0, rb, rb.at[pl.ds(0, 496)], sem, lambda copy: copy.wait_send())
    for i, buf in enumerate((gub, dnb, xb, hb)):
        sized(buf.at[pl.ds(0, 3)], send_sems.at[i], (ep, tp)).wait_send()


def body(tokens, norm_gain, gate_weight, up_weight, down_weight, expert_ids, route_weight):
    turned = (0, 2, 1)
    return pl.pallas_call(
        kernel,
        out_shape=pltpu.VMEM((HALF, TOK), BF16),
        in_specs=[pl.BlockSpec(memory_space=pl.ANY)] * 7,
        out_specs=pl.BlockSpec(memory_space=pltpu.VMEM),
        scratch_shapes=[
            pltpu.VMEM((HALF, TOK), BF16),
            pltpu.VMEM((8, 128), F32),
            pltpu.VMEM((TOPK, TOK), jnp.int32),
            pltpu.VMEM((TOPK, TOK), F32),
            pltpu.VMEM((512, 128), BF16),
            pltpu.VMEM((Q, 128, D), BF16),
            pltpu.VMEM((Q, HALF, D), BF16),
            pltpu.VMEM((Q, 256, 256), BF16),
            pltpu.VMEM((Q, Q, 128, 128), BF16),
            pltpu.VMEM((Q, 2, 256, 128), BF16),
            pltpu.VMEM((Q, 128, 128), BF16),
            pltpu.VMEM((512, 128), BF16),
            pltpu.VMEM((512, 768), BF16),
            pltpu.SemaphoreType.DMA((7,)),
            pltpu.SemaphoreType.DMA,
            pltpu.SemaphoreType.DMA((Q,)),
            pltpu.SemaphoreType.DMA,
            pltpu.SemaphoreType.DMA,
            pltpu.SemaphoreType.DMA((4,)),
            pltpu.SemaphoreType.DMA((3,)),
            pltpu.SemaphoreType.DMA((3,)),
            pltpu.SemaphoreType.DMA((N_PART,)),
            pltpu.SemaphoreType.DMA((N_PART, 3)),
        ],
        compiler_params=pltpu.CompilerParams(collective_id=0, has_side_effects=True),
    )(
        tokens.T, norm_gain.reshape(8, 128), gate_weight.transpose(turned), up_weight.transpose(turned),
        down_weight.transpose(turned), expert_ids.T, route_weight.T,
    ).T


def solution(mesh):
    in_specs = (
        P("ep", "tp"),
        P(),
        P("ep", None, "tp"),
        P("ep", None, "tp"),
        P("ep", None, "tp"),
        P("ep", None),
        P("ep", None),
    )
    return jax.shard_map(body, mesh=mesh, in_specs=in_specs, out_specs=P("ep", "tp"), check_vma=False)
```

```python
import jax
import jax.numpy as jnp
from jax import lax
from jax.experimental import pallas as pl
from jax.experimental.pallas import tpu as pltpu
from jax.sharding import PartitionSpec as P

MESH = pl.DeviceIdType.MESH
F32 = jnp.float32
BF16 = jnp.bfloat16

EPSILON = 1e-06
ALPHA = 1.702
LIMIT = 7.0

NZ = 16
Q = 4
D = 1024
TOK = 128
EXPERTS = 32
TOPK = 4
HALF = 64
Z_ORDER = (8, 7, 9, 6, 10, 5, 11, 4, 12, 3, 13, 2, 14, 1, 15, 0)
PARTS = ((0,), (1,), (2, 3))
N_PART = len(PARTS)


def iota(shape, dim):
    return lax.broadcasted_iota(jnp.int32, shape, dim)


def dot(a, b):
    return jnp.dot(a, b, preferred_element_type=F32)


def dot_rows(a, b):
    return lax.dot_general(a, b, (((1,), (1,)), ((), ())), preferred_element_type=F32)


def dot_columns(a, b):
    return lax.dot_general(a, b, (((0,), (0,)), ((), ())), preferred_element_type=F32)


def placed(offset):
    return jnp.where(iota((HALF, 128), 1) == iota((HALF, 128), 0) + offset, 1.0, 0.0).astype(BF16)


def swap(a, b):
    low = iota(a.shape, 1) < HALF
    return jnp.where(low, a, pltpu.roll(b, HALF, 1)), jnp.where(low, pltpu.roll(a, HALF, 1), b)


def bits(v):
    return v // 2, ((v + 1) % Q) // 2


def gray(a, b):
    return 3 * a + b - 2 * a * b


def place(k, quarter, column):
    if isinstance(k, int):
        a, b = (column, quarter) if k == 0 else (quarter, column)
    else:
        a = column + k * (quarter - column)
        b = quarter + k * (column - quarter)
    return gray(a // 2, b // 2) * Q + gray(a % 2, b % 2)


def rows_at(j, core):
    return (j * 2 + core) * 16


def tile(start):
    return pl.ds(start if isinstance(start, int) else pl.multiple_of(start, 16), 16)


def sized(ref, sem, device):
    return pltpu.make_async_remote_copy(
        src_ref=ref, dst_ref=ref, send_sem=sem, recv_sem=sem, device_id=device, device_id_type=MESH
    )


class Square:
    def __init__(self, view, mine, device, send_sem, recv_sems):
        self.view, self.device = view, device
        self.send_sem, self.recv_sems = send_sem, recv_sems
        self.mine = mine
        self.right = mine + 1 - 2 * (mine % 2)
        self.left = mine + 2 - 4 * (mine // 2)
        self.far = 3 - mine
        self.others = (self.far, self.right, self.left)

    def send(self, owner, h, to, index):
        pltpu.make_async_remote_copy(
            src_ref=self.view(owner, h),
            dst_ref=self.view(owner, h),
            send_sem=self.send_sem,
            recv_sem=self.recv_sems.at[index],
            device_id=self.device(to),
            device_id_type=MESH,
        ).start()

    def arrived(self, ref, index):
        sized(ref, self.recv_sems.at[index], self.device(self.right)).wait_recv()


class Gather(Square):
    def start(self):
        self.send(self.mine, 0, self.right, 0)
        self.send(self.mine, 1, self.left, 1)
        self.send(self.mine, 1, self.right, 2)
        self.send(self.mine, 0, self.left, 2)

    def forward(self):
        self.arrived(self.view(self.right, 0), 0)
        self.send(self.right, 0, self.left, 2)
        self.arrived(self.view(self.left, 1), 1)
        self.send(self.left, 1, self.right, 2)


class Exchange(Square):
    def __init__(self, *args, apart):
        super().__init__(*args)
        self.apart = apart

    def send_all(self, h):
        for index, to in enumerate(self.others):
            self.send(self.mine, h, to, index if self.apart else 0)


def kernel(
    tok_hbm, gain_hbm, gate_hbm, up_hbm, down_hbm, ids_hbm, rw_hbm, out_ref,
    tok, gain, ids, rw,
    pbuf, gub, dnb, dnf, xb, hb, ob, rb, mixer,
    in_sem, disp_send, disp_recv, ret_send, ret_recv, send_sems, gu_recv, dn_recv, x_recv, h_recv,
):
    ep = lax.axis_index("ep")
    tp = lax.axis_index("tp")
    z, c = ep // 2, ep % 2
    (ay, by), (ax, bx) = bits(tp // Q), bits(tp % Q)
    side_a, side_b = ay * 2 + ax, by * 2 + bx
    quarter_of, column_of = (side_b, side_a), (side_a, side_b)
    quarter = side_b + c * (side_a - side_b)
    column = side_a + c * (side_b - side_a)

    barrier = pltpu.get_barrier_semaphore()

    def greet(device):
        pl.semaphore_signal(barrier, inc=1, device_id=device, device_id_type=MESH)

    def with_column(to):
        return (ep, place(c, to, column))

    def with_quarter(to):
        return (ep, place(c, quarter, to))

    z_low = (z - quarter + NZ) % Q

    def is_own(j, cs):
        return jnp.logical_and(jnp.logical_and(quarter == 0, c == cs), z // Q == j)

    for j in range(Q):
        z_from = j * Q + z_low
        for cs in range(2):
            for qs in range(Q):
                device = (z_from * 2 + cs, place(c, qs, column))
                if qs == 0:
                    @pl.when(jnp.logical_not(is_own(j, cs)))
                    def _():
                        greet(device)
                else:
                    greet(device)

    loads = []
    for i, (src, dst) in enumerate(
        ((ids_hbm, ids), (tok_hbm, tok), (gate_hbm.at[0], gub.at[quarter, pl.ds(0, HALF)]),
         (up_hbm.at[0], gub.at[quarter, pl.ds(HALF, HALF)]), (down_hbm.at[0], dnb.at[quarter]),
         (gain_hbm, gain), (rw_hbm, rw))
    ):
        load = pltpu.make_async_copy(src, dst, in_sem.at[i])
        load.start()
        loads.append(load)

    gu = Gather(
        lambda o, h: gub.at[o, pl.ds(h * HALF, HALF)], quarter, with_column, send_sems.at[0], gu_recv
    )
    dn = Gather(
        lambda o, h: dnb.at[o, pl.ds(h * 32, 32)], quarter, with_column, send_sems.at[1], dn_recv
    )
    x_parts, h_parts = [], []
    for i, part in enumerate(PARTS):
        x_parts.append(Exchange(
            lambda o, h, first=part[0]: xb.at[o, :, pl.ds((first + h) * 32, 32)],
            column, with_quarter, send_sems.at[2], x_recv.at[pl.ds(i, 1)], apart=False,
        ))
        h_parts.append(Exchange(
            lambda o, h, part=part: hb.at[o, h, pl.ds(part[0] * 64, len(part) * 64)],
            column, with_quarter, send_sems.at[3], h_recv.at[i], apart=True,
        ))
    for gather in (gu, x_parts[0]):
        greet(gather.device(gather.right))
        greet(gather.device(gather.left))
    greet(x_parts[0].device(x_parts[0].far))

    loads[0].wait()
    experts = iota((EXPERTS, TOK), 0)
    named = [ids[k : k + 1, :] == experts for k in range(TOPK)]
    member = named[0] | named[1] | named[2] | named[3]
    earlier = jnp.where(iota((TOK, TOK), 0) < iota((TOK, TOK), 1), 1.0, 0.0).astype(BF16)
    slot = dot(jnp.where(member, 1.0, 0.0).astype(BF16), earlier)
    code = jnp.where(member, slot, -1.0).astype(BF16)
    expand = jnp.where(iota((512, EXPERTS), 0) // 16 == iota((512, EXPERTS), 1), 1.0, 0.0).astype(BF16)
    code_wide = dot(expand, code)
    slot_of_row = (iota((512, TOK), 0) % 16).astype(F32)
    pick_low = jnp.where(code_wide == slot_of_row, 1.0, 0.0)
    pick_high = jnp.where(code_wide == slot_of_row + 16.0, 1.0, 0.0)

    loads[1].wait()
    token_low = dot_columns(tok[...], placed(0)).astype(BF16)
    token_high = dot_columns(tok[...], placed(HALF)).astype(BF16)
    packed = dot(pick_low.astype(BF16), token_low) + dot(pick_high.astype(BF16), token_high)
    pbuf[...] = packed.astype(BF16)

    pl.semaphore_wait(barrier, 2 * NZ + 5 - jnp.where(quarter == 0, 1, 0))

    def is_mine(dz, ce):
        return jnp.logical_and(quarter == 0, c == ce) if dz == 0 else None

    def dispatch():
        for dz in Z_ORDER:
            for ce in range(2):
                e = ((z + dz) % NZ) * 2 + ce
                copy = pltpu.make_async_remote_copy(
                    src_ref=pbuf.at[tile(e * 16)],
                    dst_ref=xb.at[column_of[ce], quarter_of[ce], tile(rows_at(z // Q, c))],
                    send_sem=disp_send,
                    recv_sem=disp_recv.at[z // Q],
                    device_id=(e, place(ce, dz % Q, column_of[ce])),
                    device_id_type=MESH,
                )
                if dz == 0:
                    @pl.when(jnp.logical_not(is_mine(dz, ce)))
                    def _():
                        copy.start()

                    @pl.when(is_mine(dz, ce))
                    def _():
                        xb[column, 0, tile(rows_at(z // Q, c)), :] = pbuf[tile(e * 16), :]
                else:
                    copy.start()

    dispatch()

    for load in loads[2:5]:
        load.wait()
    gu.start()
    dn.start()

    loads[5].wait()
    loads[6].wait()
    weight = jnp.zeros((EXPERTS, TOK), F32)
    for k in range(TOPK):
        weight = weight + jnp.where(named[k], rw[k : k + 1, :], 0.0)
    for i in range(3):
        piece = weight.astype(BF16)
        weight = weight - piece.astype(F32)
        wide = dot(expand, piece)
        mixer[:, i * 128 : i * 128 + 128] = (wide * pick_low).astype(BF16)
        mixer[:, 384 + i * 128 : 512 + i * 128] = (wide * pick_high).astype(BF16)

    gu.forward()
    dn.forward()

    def all_but_own(own, whole, rest, sem, wait):
        @pl.when(jnp.logical_not(own))
        def _():
            wait(sized(whole, sem, (ep, tp)))

        @pl.when(own)
        def _():
            wait(sized(rest, sem, (ep, tp)))

    def pass_rows(part):
        for h, j in enumerate(PARTS[part]):
            all_but_own(
                jnp.logical_and(quarter == 0, z // Q == j),
                xb.at[column, :, pl.ds(j * 32, 32)], pbuf.at[pl.ds(0, 112)],
                disp_recv.at[j], lambda copy: copy.wait_recv(),
            )
            x_parts[part].send_all(h)

    def x_arrived(part):
        js = PARTS[part]
        x_parts[part].arrived(xb.at[pl.ds(0, 3), :, pl.ds(js[0] * 32, len(js) * 32)], 0)

    def slice_at(s, part):
        (ty, uy), (tx, ux) = bits(s // Q), bits(s % Q)
        t, u = ty * 2 + tx, uy * 2 + ux
        first, last = PARTS[part][0] * 32, PARTS[part][-1] * 32 + 32
        return xb[t + c * (u - t), u + c * (t - u), first:last].astype(F32)

    def make_hidden(part):
        groups = []
        at, count = PARTS[part][0] * 64, len(PARTS[part]) * 64
        square = jnp.zeros((count, 128), F32)
        for g in range(8):
            low, high = swap(slice_at(2 * g, part), slice_at(2 * g + 1, part))
            both = jnp.concatenate([low, high], axis=0)
            square = square + both * both
            groups.append(both)
        inverse = lax.rsqrt(jnp.sum(square, axis=1, keepdims=True) / D + EPSILON)
        rows = jnp.concatenate(
            [(groups[g] * inverse * gain[g : g + 1, :]).astype(BF16) for g in range(8)], axis=1
        )
        for p in range(2):
            both = dot_rows(rows, jnp.concatenate([gub[2 * p], gub[2 * p + 1]], axis=0))
            gate_pre, up_pre = swap(both[:, :128], both[:, 128:])
            gate_pre = jnp.minimum(gate_pre, LIMIT)
            up_pre = jnp.clip(up_pre, -LIMIT, LIMIT)
            hidden = (up_pre + 1.0) * gate_pre * jax.nn.sigmoid(ALPHA * gate_pre)
            hb[column, p, at : at + count] = hidden.astype(BF16)
            h_parts[part].send_all(p)

    def order_down(k):
        low = iota((HALF, 128), 1) < HALF
        for n in range(Q):
            for o in range(Q):
                for p in range(2):
                    sides = []
                    for h in range(2):
                        s = place(k, 2 * p + h, o)
                        v = dnb[n, :, s // 2 * 128 : s // 2 * 128 + 128].astype(F32)
                        sides.append(v if s % 2 == h else pltpu.roll(v, HALF, 1))
                    dnf[o, n * HALF : n * HALF + HALF, p * 128 : p * 128 + 128] = jnp.where(low, *sides).astype(BF16)

    def make_result(part):
        exchange = h_parts[part]
        at, count = PARTS[part][0] * 32, len(PARTS[part]) * 32

        def term(owner):
            units = jnp.concatenate([hb[owner, p, 2 * at : 2 * at + 2 * count] for p in range(2)], axis=1)
            return dot_rows(units, dnf[owner])

        result = term(column)
        for index in (1, 2, 0):
            owner = exchange.others[index]
            exchange.arrived(hb.at[owner, :, pl.ds(2 * at, 2 * count)], index)
            result = result + term(owner)
        for n in range(2):
            cols = result[:, n * 128 : n * 128 + 128]
            pair = swap(cols[:count], cols[count:])
            ob[2 * n, at : at + count], ob[2 * n + 1, at : at + count] = [v.astype(BF16) for v in pair]
            send_back(part, (2 * n, 2 * n + 1))

    def send_back(part, quarters):
        for j in PARTS[part]:
            z_to = j * Q + z_low
            for cs in range(2):
                for qs in quarters:
                    copy = pltpu.make_async_remote_copy(
                        src_ref=ob.at[qs, tile(rows_at(j, cs))],
                        dst_ref=rb.at[tile(ep * 16)],
                        send_sem=ret_send,
                        recv_sem=ret_recv,
                        device_id=(z_to * 2 + cs, place(c, qs, column)),
                        device_id_type=MESH,
                    )
                    if qs == 0:
                        own = is_own(j, cs)

                        @pl.when(jnp.logical_not(own))
                        def _():
                            copy.start()

                        @pl.when(own)
                        def _():
                            rb[tile(ep * 16), :] = ob[0, tile(rows_at(j, cs)), :]
                    else:
                        copy.start()

    pass_rows(0)
    pass_rows(1)
    pass_rows(2)
    dn.arrived(dnb.at[pl.ds(0, 2)], 2)
    for k in range(2):
        @pl.when(c == k)
        def _():
            order_down(k)
    x_arrived(0)
    gu.arrived(gub.at[pl.ds(0, 2)], 2)
    make_hidden(0)
    x_arrived(1)
    make_hidden(1)
    x_arrived(2)
    make_hidden(2)
    make_result(0)
    make_result(1)
    make_result(2)

    all_but_own(
        quarter == 0, rb, rb.at[pl.ds(0, 496)], ret_recv, lambda copy: copy.wait_recv()
    )

    mixed = dot_columns(rb[...], mixer[...])
    combined = mixed[0:HALF, 0:128] + mixed[HALF:128, 384:512]
    for i in range(1, 3):
        combined = combined + mixed[0:HALF, i * 128 : i * 128 + 128]
        combined = combined + mixed[HALF:128, 384 + i * 128 : 512 + i * 128]
    out_ref[...] = combined.astype(BF16)

    for sem in (disp_send, ret_send):
        all_but_own(quarter == 0, rb, rb.at[pl.ds(0, 496)], sem, lambda copy: copy.wait_send())
    for i, buf in enumerate((gub, dnb, xb, hb)):
        sized(buf.at[pl.ds(0, 3)], send_sems.at[i], (ep, tp)).wait_send()


def body(tokens, norm_gain, gate_weight, up_weight, down_weight, expert_ids, route_weight):
    turned = (0, 2, 1)
    return pl.pallas_call(
        kernel,
        out_shape=pltpu.VMEM((HALF, TOK), BF16),
        in_specs=[pl.BlockSpec(memory_space=pl.ANY)] * 7,
        out_specs=pl.BlockSpec(memory_space=pltpu.VMEM),
        scratch_shapes=[
            pltpu.VMEM((HALF, TOK), BF16),
            pltpu.VMEM((8, 128), F32),
            pltpu.VMEM((TOPK, TOK), jnp.int32),
            pltpu.VMEM((TOPK, TOK), F32),
            pltpu.VMEM((512, 128), BF16),
            pltpu.VMEM((Q, 128, D), BF16),
            pltpu.VMEM((Q, HALF, D), BF16),
            pltpu.VMEM((Q, 256, 256), BF16),
            pltpu.VMEM((Q, Q, 128, 128), BF16),
            pltpu.VMEM((Q, 2, 256, 128), BF16),
            pltpu.VMEM((Q, 128, 128), BF16),
            pltpu.VMEM((512, 128), BF16),
            pltpu.VMEM((512, 768), BF16),
            pltpu.SemaphoreType.DMA((7,)),
            pltpu.SemaphoreType.DMA,
            pltpu.SemaphoreType.DMA((Q,)),
            pltpu.SemaphoreType.DMA,
            pltpu.SemaphoreType.DMA,
            pltpu.SemaphoreType.DMA((4,)),
            pltpu.SemaphoreType.DMA((3,)),
            pltpu.SemaphoreType.DMA((3,)),
            pltpu.SemaphoreType.DMA((N_PART,)),
            pltpu.SemaphoreType.DMA((N_PART, 3)),
        ],
        compiler_params=pltpu.CompilerParams(collective_id=0, has_side_effects=True),
    )(
        tokens.T, norm_gain.reshape(8, 128), gate_weight.transpose(turned), up_weight.transpose(turned),
        down_weight.transpose(turned), expert_ids.T, route_weight.T,
    ).T


def solution(mesh):
    in_specs = (
        P("ep", "tp"),
        P(),
        P("ep", None, "tp"),
        P("ep", None, "tp"),
        P("ep", None, "tp"),
        P("ep", None),
        P("ep", None),
    )
    return jax.shard_map(body, mesh=mesh, in_specs=in_specs, out_specs=P("ep", "tp"), check_vma=False)
```
